256 devices in a mesh: sp: 64 (over z, x, core), tp: 4 (over y).
Axes of the slice: x: 4, y: 4, z: 8, core: 2. Of those that a mesh axis runs over, the one named last changes fastest.
Arguments:
- queries: bfloat16 [16384, 1024], P('sp', 'tp'), may hold values from -9 to 9
- keys: bfloat16 [16384, 512], P('sp', 'tp'), may hold values from -9 to 9
- values: bfloat16 [16384, 512], P('sp', 'tp'), may hold values from -6 to 6
- residual: bfloat16 [16384, 2048], P(('sp', 'tp')), may hold values from -6 to 6
- query_gain: float32 [128], replicated, may hold values from 1 to 5
- key_gain: float32 [128], replicated, may hold values from 1 to 5
- out_weight: bfloat16 [1024, 2048], replicated, may hold values from -0.1875 to 0.1875
- first_gain: float32 [2048], replicated, may hold values from 0.1 to 1.9
- first_bias: float32 [2048], replicated, may hold values from -3 to 3
- up_weight: bfloat16 [2048, 8192], P('sp', 'tp'), may hold values from -0.125 to 0.125
- down_weight: bfloat16 [2048, 8192], P('sp', 'tp'), may hold values from -0.0625 to 0.0625
- second_gain: float32 [2048], replicated, may hold values from 0.1 to 1.9
- second_bias: float32 [2048], replicated, may hold values from -3 to 3
Outputs:
- layer_out: bfloat16 [16384, 2048], P(('sp', 'tp'))
The draws below stay inside these ranges and needn't reach their ends.
All inputs are finite; a program needn't handle non-finite values.
Results may differ from the reference program's by a relative error of at most 0.015.
Values may be sent and summed in bfloat16 or wider, within the bound.
A program may use at most 128 MiB of HBM per device.

```python
import math
import jax
import jax.numpy as jnp
from jax import lax

D = 2048
HEADS = 8
KV_HEADS = 4
HEAD_DIM = 128
FF = 8192
GRID_W = 64
TOKENS = 16384


def draw_queries(key, part):
    noise = jnp.clip(jax.random.normal(jax.random.fold_in(key, 1), (TOKENS, HEADS * HEAD_DIM), jnp.float32), -6.0, 6.0)
    return noise.astype(jnp.bfloat16)


def draw_keys(key, part):
    noise = jnp.clip(jax.random.normal(jax.random.fold_in(key, 2), (TOKENS, KV_HEADS * HEAD_DIM), jnp.float32), -6.0, 6.0)
    return noise.astype(jnp.bfloat16)


def level_of(stream_key, shape, shards, smallest, top_value):
    level, own = 1.0, jax.random.fold_in(stream_key, 6)
    for axis_at, blocks in shards:
        heights = jnp.exp(jax.random.uniform(jax.random.fold_in(own, axis_at), (blocks,), jnp.float32, smallest / len(shards), top_value / len(shards)))
        level = level * jnp.repeat(heights, shape[axis_at] // blocks).reshape([-1 if axis == axis_at else 1 for axis in range(len(shape))])
    return level


def bell_draw(key, extent, width, limit, cuts=(), held_as=jnp.bfloat16):
    values = jax.random.normal(key, extent, jnp.float32) * width
    if len(cuts) > 0:
        values = level_of(key, extent, cuts, -0.22, 0.18) * values
    return jnp.clip(values, min=-limit, max=limit).astype(held_as)


def setup_inputs(seed: int = 0) -> dict:
    streams_of = jax.random.split(jax.random.key(seed), 14)
    queries = draw_queries(jax.random.fold_in(streams_of[13], 71), 0)
    keys = draw_keys(jax.random.fold_in(streams_of[13], 71), 0)
    values = bell_draw(streams_of[2], (TOKENS, KV_HEADS * HEAD_DIM), 1.0, 6.0, ((0, 64), (1, 4)))
    residual = bell_draw(streams_of[3], (TOKENS, D), 1.0, 6.0, ((0, 256),))
    query_gain = jnp.clip(jax.random.uniform(streams_of[4], (HEAD_DIM,), jnp.float32, 1.0, 5.0), 1.0, 5.0)
    key_gain = jnp.clip(jax.random.uniform(streams_of[5], (HEAD_DIM,), jnp.float32, 1.0, 5.0), 1.0, 5.0)
    out_weight = bell_draw(streams_of[6], (HEADS * HEAD_DIM, D), (HEADS * HEAD_DIM) ** -0.5, 0.1875)
    first_gain = jnp.clip(1.0 + 0.18 * jax.random.normal(streams_of[7], (D,), jnp.float32), 0.1, 1.9)
    first_bias = bell_draw(streams_of[8], (D,), 0.5, 3.0, (), jnp.float32)
    up_weight = bell_draw(streams_of[9], (D, FF), D ** -0.5, 0.125, ((0, 64), (1, 4)))
    down_weight = bell_draw(streams_of[10], (D, FF), FF ** -0.5, 0.0625, ((0, 64), (1, 4)))
    second_gain = jnp.clip(1.0 + 0.18 * jax.random.normal(streams_of[11], (D,), jnp.float32), 0.1, 1.9)
    second_bias = bell_draw(streams_of[12], (D,), 0.5, 3.0, (), jnp.float32)
    return dict(queries=queries, keys=keys, values=values, residual=residual, query_gain=query_gain, key_gain=key_gain, out_weight=out_weight, first_gain=first_gain, first_bias=first_bias, up_weight=up_weight, down_weight=down_weight, second_gain=second_gain, second_bias=second_bias)


RESIDUAL_SCALE = 2.0 ** 0.25
LAYER_EPS = 1e-05
HEAD_EPS = 1e-06
ROTARY_BASE = 10000.0

def grid_angles(positions, head_dim):
    quarter = head_dim // 4
    inverse = ROTARY_BASE ** (-jnp.arange(quarter, dtype=jnp.float32) / quarter)
    grid_row = (positions // GRID_W).astype(jnp.float32)
    grid_col = (positions % GRID_W).astype(jnp.float32)
    return jnp.concatenate([grid_row[:, None] * inverse, grid_col[:, None] * inverse], axis=-1)

def norm_rotate(projected, gain, angles, head_dim):
    row_count = projected.shape[0]
    head_count = projected.shape[1] // head_dim
    as_float = projected.astype(jnp.float32).reshape(row_count, head_count, head_dim)
    normed = as_float * lax.rsqrt(lax.optimization_barrier(jnp.mean(as_float * as_float, axis=-1, keepdims=True)) + HEAD_EPS) * gain
    paired = normed.reshape(row_count, head_count, head_dim // 2, 2)
    cosine = jnp.cos(angles)[:, None, :]
    sine = jnp.sin(angles)[:, None, :]
    even_part = paired[..., 0]
    odd_part = paired[..., 1]
    turned = jnp.stack([even_part * cosine - odd_part * sine, even_part * sine + odd_part * cosine], axis=-1)
    return turned.reshape(row_count, head_count, head_dim).astype(jnp.bfloat16)

def layer_norm(summed, gain, bias):
    centred = summed - lax.optimization_barrier(jnp.mean(summed, axis=-1, keepdims=True))
    variance = lax.optimization_barrier(jnp.mean(centred * centred, axis=-1, keepdims=True))
    return centred * lax.rsqrt(variance + LAYER_EPS) * gain + bias

def reference(queries, keys, values, residual, query_gain, key_gain, out_weight, first_gain, first_bias, up_weight, down_weight, second_gain, second_bias):
    positions = jnp.arange(TOKENS, dtype=jnp.int32)
    angles = grid_angles(positions, HEAD_DIM)
    query_rot = norm_rotate(queries, query_gain, angles, HEAD_DIM)
    key_float = norm_rotate(keys, key_gain, angles, HEAD_DIM).astype(jnp.float32)
    value_rows = values.reshape(TOKENS, KV_HEADS, HEAD_DIM).astype(jnp.float32)
    group = HEADS // KV_HEADS
    block_rows = math.gcd(TOKENS, 256)
    score_scale = HEAD_DIM ** (-0.5)

    def one_block(begin):
        query_block = lax.dynamic_slice_in_dim(query_rot, begin, block_rows, 0).astype(jnp.float32)
        query_block = query_block.reshape(block_rows, KV_HEADS, group, HEAD_DIM)
        scores = jnp.einsum('qkgd,skd->kgqs', query_block, key_float) * score_scale
        largest = lax.optimization_barrier(jnp.max(scores, axis=-1, keepdims=True))
        weights = jnp.exp(scores - largest)
        total = lax.optimization_barrier(jnp.sum(weights, axis=-1))
        rounded = lax.optimization_barrier(weights.astype(jnp.bfloat16)).astype(jnp.float32)
        summed = jnp.einsum('kgqs,skd->kgqd', rounded, value_rows)
        result = summed / total[..., None]
        return jnp.transpose(result, (2, 0, 1, 3)).reshape(block_rows, HEADS * HEAD_DIM).astype(jnp.bfloat16)
    starts = jnp.arange(TOKENS // block_rows, dtype=jnp.int32) * block_rows
    attended = lax.map(one_block, starts).reshape(TOKENS, HEADS * HEAD_DIM)
    mixed = jnp.dot(attended, out_weight, preferred_element_type=jnp.float32)
    first_norm = layer_norm(RESIDUAL_SCALE * residual.astype(jnp.float32) + mixed, first_gain, first_bias).astype(jnp.bfloat16)
    up_values = jnp.dot(first_norm, up_weight, preferred_element_type=jnp.float32)
    hidden = jnp.square(jnp.maximum(up_values, 0.0)).astype(jnp.bfloat16)
    channel_out = lax.dot_general(hidden, down_weight, (((1,), (1,)), ((), ())), preferred_element_type=jnp.float32)
    layer_out = layer_norm(RESIDUAL_SCALE * first_norm.astype(jnp.float32) + channel_out, second_gain, second_bias)
    return layer_out.astype(jnp.bfloat16)
```

```python
import functools

import jax
import jax.numpy as jnp
import numpy as np
from jax import lax
from jax.experimental import pallas as pl
from jax.experimental.pallas import tpu as pltpu
from jax.sharding import PartitionSpec as P

MESH = pl.DeviceIdType.MESH
HEAD_DIM = 128
GRID_W = 64
RESIDUAL_SCALE = 2.0**0.25
LAYER_EPS = 1e-05
HEAD_EPS = 1e-06
ROTARY_BASE = 10000.0
NZ, NX, NC, NY = 8, 4, 2, 4
SCALE2 = float(np.log2(np.e) * HEAD_DIM**-0.5)
AW = 640
W_COLS = 1024
PASS1 = 3 * 512
KEYS = 4096
F32, BF16 = jnp.float32, jnp.bfloat16


def rotary_tables():
    inverse = (np.float32(ROTARY_BASE) ** (-np.arange(32, dtype=np.float32) / np.float32(32))).astype(np.float32)
    ang = np.arange(256, dtype=np.float32)[:, None] * inverse
    sign = np.tile(np.array([-1.0, 1.0], np.float32), 32)
    cos = np.repeat(np.cos(ang), 2, axis=1).astype(np.float32)
    sin = np.repeat(np.sin(ang), 2, axis=1).astype(np.float32) * sign
    return cos, sin


class Copy:
    def __init__(self, pool, src, dst, land, dev):
        self.n = pool.take()
        self.pool, self.src, self.dst, self.land, self.dev = pool, src, dst, land, dev

    def start(self):
        self._make(self.src(), self.dst()).start()

    def wait(self):
        here = self.land()
        self._make(here, here).wait_recv()

    def drain(self):
        src = self.src()
        self._make(src, self.dst()).wait_send()

    def _make(self, src, dst):
        return pltpu.make_async_remote_copy(
            src_ref=src, dst_ref=dst, send_sem=self.pool.ssem.at[self.n], recv_sem=self.pool.rsem.at[self.n],
            device_id=self.dev, device_id_type=MESH,
        )


class Pool:
    def __init__(self, ssem, rsem, size):
        self.ssem, self.rsem, self.size, self.n, self.all = ssem, rsem, size, 0, []

    def take(self):
        self.n += 1
        assert self.n <= self.size
        return self.n - 1

    def copy(self, src, dst, land, dev):
        c = Copy(self, src, dst, land, dev)
        self.all.append(c)
        return c


N_SEMS = 192


def layer_norm(summed, gain, bias):
    centred = summed - jnp.mean(summed, axis=-1, keepdims=True)
    variance = jnp.mean(centred * centred, axis=-1, keepdims=True)
    return centred * lax.rsqrt(variance + LAYER_EPS) * gain + bias


def norm_rotate(x, gain, cos, sin):
    x = x.astype(F32)
    x = x * lax.rsqrt(jnp.mean(x * x, axis=-1, keepdims=True) + HEAD_EPS) * gain
    even = lax.broadcasted_iota(jnp.int32, x.shape, 1) % 2 == 0
    swapped = jnp.where(even, pltpu.roll(x, HEAD_DIM - 1, 1), pltpu.roll(x, 1, 1))
    return (x * cos + swapped * sin).astype(BF16)


def eye128():
    return lax.broadcasted_iota(jnp.int32, (128, 128), 0) == lax.broadcasted_iota(jnp.int32, (128, 128), 1)


def dot(a, b, dims=((1,), (0,))):
    return lax.dot_general(a, b, (dims, ((), ())), preferred_element_type=F32)


def kernel(
    q_ref, k_ref, v_ref, cos_ref, sin_ref, qg_ref, kg_ref, fg_ref, fb_ref, sg_ref, sb_ref,
    res_hbm, ow_hbm, up_hbm, dn_hbm,
    out_ref,
    kvbuf, qbuf, o_acc, m_acc, l_acc, s_scr, osend, orecv, stsend, strecv, att_s, attbuf, ow, res, xbuf,
    upbuf, dnbuf, hid, psend, precv, pown, ysend, yrecv, fin,
    ssem, rsem, lsem,
):
    sp, y = lax.axis_index("sp"), lax.axis_index("tp")
    z, x, c = sp // 8, (sp // 2) % 4, sp % 2
    pool = Pool(ssem, rsem, N_SEMS)

    def dev(dz=0, dx=0, dy=0, flip=False):
        zz, xx, yy = (z + dz + NZ) % NZ, (x + dx + NX) % NX, (y + dy + NY) % NY
        cc = 1 - c if flip else c
        return (zz * 8 + xx * 2 + cc, yy)

    def zat(d):
        return (z + d + NZ) % NZ

    def xat(d):
        return (x + d + NX) % NX

    barrier = pltpu.get_barrier_semaphore()
    partners = [dict(dz=1), dict(dz=-1), dict(dx=1), dict(dx=-1), dict(dx=2), dict(dy=1), dict(dy=-1), dict(dy=2), dict(flip=True)]
    for p in partners:
        pl.semaphore_signal(barrier, inc=1, device_id=dev(**p), device_id_type=MESH)

    def block(zs, xs):
        return pl.multiple_of(zs * 256 + xs * 64, 64)

    mine = pl.multiple_of(c * W_COLS, W_COLS)
    other = pl.multiple_of((1 - c) * W_COLS, W_COLS)
    my_rows = pl.ds(pl.multiple_of(block(z, x) + c * 32, 32), 32)
    partner_rows = pl.ds(pl.multiple_of(block(z, x) + (1 - c) * 32, 32), 32)
    local = [
        pltpu.make_async_copy(up_hbm.at[:, pl.ds(mine, W_COLS)], upbuf.at[my_rows, :], lsem.at[0]),
        pltpu.make_async_copy(dn_hbm.at[:, pl.ds(mine, W_COLS)], dnbuf.at[my_rows, :], lsem.at[1]),
        pltpu.make_async_copy(ow_hbm, ow, lsem.at[2]),
        pltpu.make_async_copy(res_hbm, res, lsem.at[3]),
    ]
    for l in local:
        l.start()

    cos, sin = cos_ref[...], sin_ref[...]
    kvbuf[0:256, 0:128] = norm_rotate(k_ref[...], kg_ref[...], cos, sin)
    kvbuf[0:256, 128:256] = v_ref[...]
    qbuf[0:256, :] = norm_rotate(q_ref[:, 0:128], qg_ref[...], cos, sin)
    qbuf[256:512, :] = norm_rotate(q_ref[:, 128:256], qg_ref[...], cos, sin)

    def same(ref, rows, cols, land_rows, device):
        view = lambda: ref.at[pl.ds(*rows), pl.ds(*cols)]
        return pool.copy(view, view, lambda: ref.at[pl.ds(*land_rows), pl.ds(*cols)], device)

    flip = dev(flip=True)
    KP, KM, KD = {}, {}, {}
    full = (0, 256)
    for s in range(1, 5):
        lo, n = (0, 256) if s < 4 else (0, 128)
        src = 0 if s == 1 else 2 * (s - 1) - 1
        dst = 2 * s - 1
        KP[s] = pool.copy(
            lambda src=src, lo=lo, n=n: kvbuf.at[pl.ds(src * 512 + lo, n), :],
            lambda dst=dst, lo=lo, n=n: kvbuf.at[pl.ds(dst * 512 + lo, n), :],
            lambda dst=dst, lo=lo, n=n: kvbuf.at[pl.ds(dst * 512 + lo, n), :], dev(dz=1))
        lo = 0 if s < 4 else 128
        src = 0 if s == 1 else 2 * (s - 1)
        dst = 2 * s if s < 4 else 7
        KM[s] = pool.copy(
            lambda src=src, lo=lo, n=n: kvbuf.at[pl.ds(src * 512 + lo, n), :],
            lambda dst=dst, lo=lo, n=n: kvbuf.at[pl.ds(dst * 512 + lo, n), :],
            lambda dst=dst, lo=lo, n=n: kvbuf.at[pl.ds(dst * 512 + lo, n), :], dev(dz=-1))
    for j in range(8):
        KD[j] = pool.copy(
            lambda j=j: kvbuf.at[pl.ds(j * 512, 256), :],
            lambda j=j: kvbuf.at[pl.ds(j * 512 + 256, 256), :],
            lambda j=j: kvbuf.at[pl.ds(j * 512 + 256, 256), :], flip)
    QS, OS, ST, AT = {}, {}, {}, {}
    for d in range(1, 4):
        QS[d] = pool.copy(
            lambda: qbuf.at[pl.ds(0, 512), :], lambda d=d: qbuf.at[pl.ds(d * 512, 512), :],
            lambda d=d: qbuf.at[pl.ds(d * 512, 512), :], dev(dx=d))
        OS[d] = pool.copy(lambda d=d: osend.at[d], lambda d=d: orecv.at[d], lambda d=d: orecv.at[d], dev(dx=-d))
        ST[d] = pool.copy(lambda d=d: stsend.at[d], lambda d=d: strecv.at[d], lambda d=d: strecv.at[d], dev(dx=-d))
        AT[d] = pool.copy(
            lambda d=d: att_s.at[pl.ds(pl.multiple_of((y + d) % NY * 64, 64), 64), :],
            lambda d=d: attbuf.at[d], lambda d=d: attbuf.at[d], dev(dy=d))
    def rows_of(ref, lo, n):
        return lambda: ref.at[pl.ds(lo, n), :]

    YP1 = pool.copy(rows_of(xbuf, 0, 64), rows_of(xbuf, 64, 64), rows_of(xbuf, 64, 64), dev(dy=1))
    YM1 = pool.copy(rows_of(xbuf, 0, 64), rows_of(xbuf, 192, 64), rows_of(xbuf, 192, 64), dev(dy=-1))
    YP2 = pool.copy(rows_of(xbuf, 64, 32), rows_of(xbuf, 128, 32), rows_of(xbuf, 128, 32), dev(dy=1))
    YM2 = pool.copy(rows_of(xbuf, 224, 32), rows_of(xbuf, 160, 32), rows_of(xbuf, 160, 32), dev(dy=-1))
    XD = [pool.copy(rows_of(xbuf, j * 64, 64), rows_of(xbuf, 256 + j * 64, 64), rows_of(xbuf, 256 + j * 64, 64), flip) for j in range(4)]

    def exchange(hbm, buf):
        return pool.copy(
            lambda: hbm.at[:, pl.ds(other, W_COLS)], lambda: buf.at[my_rows, :], lambda: buf.at[partner_rows, :], flip)

    WX = {"u": exchange(up_hbm, upbuf), "d": exchange(dn_hbm, dnbuf)}
    order = [0, -1, 1, -2, 2, -3, 3, 4]

    class Gather:
        def __init__(self, buf):
            a, b = (0, AW), (AW, W_COLS - AW)
            up, down, right, left = dev(dz=1), dev(dz=-1), dev(dx=1), dev(dx=-1)
            self.AP, self.AM, self.BP, self.BM = {}, {}, {}, {}
            for s in range(1, 5):
                n, m = (64, 256) if s < 4 else (32, 128)
                h, g = (0, 0) if s < 4 else (32, 128)
                self.AP[s] = same(buf, (block(zat(1 - s), x), n), a, (block(zat(-s), x), n), up)
                self.AM[s] = same(buf, (block(zat(s - 1), x) + h, n), a, (block(zat(s), x) + h, n), down)
                self.BP[s] = same(buf, (block(zat(1 - s), 0), m), b, (block(zat(-s), 0), m), up)
                self.BM[s] = same(buf, (block(zat(s - 1), 0) + g, m), b, (block(zat(s), 0) + g, m), down)
            self.ax = {d: self.spread(buf, zat(d), a, right, left) for d in order}
            self.bx = self.spread(buf, z, b, right, left)

        def spread(self, buf, zs, cols, right, left):
            return (
                same(buf, (block(zs, x), 64), cols, (block(zs, xat(-1)), 64), right),
                same(buf, (block(zs, x), 64), cols, (block(zs, xat(1)), 64), left),
                same(buf, (block(zs, xat(-1)), 32), cols, (block(zs, xat(-2)), 32), right),
                same(buf, (block(zs, xat(1)) + 32, 32), cols, (block(zs, xat(2)) + 32, 32), left),
            )

        def begin(self):
            for t in (self.bx[0], self.bx[1], self.AP[1], self.AM[1], self.ax[0][0], self.ax[0][1]):
                t.start()

        def pass_on(self, sp4):
            sp4[0].wait()
            sp4[2].start()
            sp4[1].wait()
            sp4[3].start()

        def first_x(self):
            self.pass_on(self.bx)
            self.pass_on(self.ax[0])

        def row(self):
            self.bx[2].wait()
            self.bx[3].wait()
            self.BP[1].start()
            self.BM[1].start()

        def a_step(self, s):
            self.AP[s].wait()
            if s < 4:
                self.AP[s + 1].start()
            self.AM[s].wait()
            if s < 4:
                self.AM[s + 1].start()
            for d in (-s, s) if s < 4 else (4,):
                self.ax[d][0].start()
                self.ax[d][1].start()

        def b_step(self, s):
            self.BP[s].wait()
            if s < 4:
                self.BP[s + 1].start()
            self.BM[s].wait()
            if s < 4:
                self.BM[s + 1].start()

        def x_step(self, s):
            for d in (-s, s) if s < 4 else (4,):
                self.pass_on(self.ax[d])

        def have(self, d):
            self.ax[d][2].wait()
            self.ax[d][3].wait()

        def events(self):
            steps = [self.begin, self.first_x, self.row]
            for s in range(1, 4):
                steps += [functools.partial(self.a_step, s), functools.partial(self.b_step, s), functools.partial(self.x_step, s)]
            return steps + [functools.partial(self.a_step, 4), functools.partial(self.b_step, 4), functools.partial(self.x_step, 4)]

    U, D = Gather(upbuf), Gather(dnbuf)
    DD = [pool.copy(lambda j=j: psend.at[j], lambda j=j: precv.at[j], lambda j=j: precv.at[j], flip) for j in range(8)]
    RS = [
        [pool.copy(lambda j=j, k=k: ysend.at[j, k], lambda j=j, k=k: yrecv.at[j, k], lambda j=j, k=k: yrecv.at[j, k], dev(dy=-k)) for k in (1, 2, 3)]
        for j in range(8)
    ]

    u, d = U.events(), D.events()
    queue = u[0:6] + [d[0]] + u[6:9] + d[1:3] + u[9:12] + d[3:6] + u[12:15] + d[6:15]
    at = [0]

    def w(n):
        for e in queue[at[0] : at[0] + n]:
            e()
        at[0] += n

    pl.semaphore_wait(barrier, len(partners))
    KP[1].start()
    KM[1].start()
    KD[0].start()
    for i in (1, 3, 2):
        QS[i].start()
    WX["u"].start()
    WX["d"].start()
    local[0].wait()
    WX["u"].wait()
    w(1)
    local[1].wait()
    WX["d"].wait()
    KP[1].wait()
    KP[2].start()
    KD[1].start()
    KM[1].wait()
    KM[2].start()
    KD[2].start()
    for i in range(3):
        KD[i].wait()
    w(1)
    for i in (1, 2, 3):
        QS[i].wait()

    def kv_step(s):
        KP[s].wait()
        KM[s].wait()
        if s < 4:
            KP[s + 1].start()
            KM[s + 1].start()
            KD[2 * s - 1].start()
            KD[2 * s].start()
        else:
            KD[7].start()

    def scores(row, lo, hi):
        q = qbuf[pl.ds(row, 256), :]
        best = None
        for at_key in range(lo, hi, 512):
            part = dot(q, kvbuf[pl.ds(at_key, 512), 0:128], ((1,), (1,)))
            s_scr[:, pl.ds(at_key - lo, 512)] = part
            for g in range(0, 512, 128):
                best = part[:, g : g + 128] if best is None else jnp.maximum(best, part[:, g : g + 128])
        return jnp.max(best, axis=1, keepdims=True)

    def weigh(m, lo, hi):
        total, out = None, None
        for at_key in range(lo, hi, 512):
            p = jnp.exp2((s_scr[:, pl.ds(at_key - lo, 512)] - m) * SCALE2)
            for g in range(0, 512, 128):
                total = p[:, g : g + 128] if total is None else total + p[:, g : g + 128]
            o = dot(p.astype(BF16), kvbuf[pl.ds(at_key, 512), 128:256])
            out = o if out is None else out + o
        return jnp.sum(total, axis=1, keepdims=True), out

    def events_at(i, table):
        for step, fns in table.items():
            @pl.when(i == step)
            def _(fns=fns):
                for f in fns:
                    f()

    def pass1(i, _):
        row = pl.multiple_of((i + 2) % 8 * 256, 256)
        m = scores(row, 0, PASS1)
        l, o = weigh(m, 0, PASS1)
        o_acc[pl.ds(row, 256), :] = o
        m_acc[pl.ds(row, 256), :] = jnp.broadcast_to(m, (256, 128))
        l_acc[pl.ds(row, 256), :] = jnp.broadcast_to(l, (256, 128))
        events_at(i, ev1)
        return 0

    def grab(n):
        got = queue[at[0] : at[0] + n]
        at[0] += n
        return got

    ev1 = {1: [lambda: kv_step(2)], 2: grab(1), 4: [lambda: kv_step(3)] + grab(1), 6: grab(1), 7: grab(1) + [lambda: kv_step(4)]}
    lax.fori_loop(0, 8, pass1, 0)
    for i in range(3, 8):
        KD[i].wait()

    def send_o(d):
        eye = eye128()
        for g in range(4):
            rows = pl.ds(d * 512 + g * 128, 128)
            stsend[d, g : g + 1, :] = jnp.sum(jnp.where(eye, m_acc[rows, :], 0.0), axis=0, keepdims=True)
            stsend[d, g + 4 : g + 5, :] = jnp.sum(jnp.where(eye, l_acc[rows, :], 0.0), axis=0, keepdims=True)
        OS[d].start()
        ST[d].start()

    def pass2(i, _):
        row = pl.multiple_of((i + 2) % 8 * 256, 256)
        m_old = m_acc[pl.ds(row, 256), 0:1]
        m = jnp.maximum(scores(row, PASS1, KEYS), m_old)
        alpha = jnp.exp2((m_old - m) * SCALE2)
        l, o = weigh(m, PASS1, KEYS)
        o = o_acc[pl.ds(row, 256), :] * alpha + o
        l = l_acc[pl.ds(row, 256), 0:1] * alpha + l
        o_acc[pl.ds(row, 256), :] = o
        m_acc[pl.ds(row, 256), :] = jnp.broadcast_to(m, (256, 128))
        l_acc[pl.ds(row, 256), :] = jnp.broadcast_to(l, (256, 128))
        osend[row // 512, pl.ds(pl.multiple_of(row % 512, 256), 256), :] = o.astype(BF16)
        events_at(i, ev2)
        return 0

    ev2 = {
        0: grab(1), 1: [lambda: send_o(1)], 2: grab(1), 3: [lambda: send_o(2)] + grab(1), 4: grab(1), 5: [lambda: send_o(3)], 6: grab(1), 7: grab(1),
    }
    lax.fori_loop(0, 8, pass2, 0)

    for i in (1, 2, 3):
        ST[i].wait()
    for i in (1, 2, 3):
        OS[i].wait()
    eye = eye128()
    for g in range(4):
        rows = pl.ds(g * 128, 128)
        ms, ls = [m_acc[rows, 0:1]], [l_acc[rows, 0:1]]
        for i in (1, 2, 3):
            ms.append(jnp.sum(jnp.where(eye, strecv[i, g : g + 1, :], 0.0), axis=1, keepdims=True))
            ls.append(jnp.sum(jnp.where(eye, strecv[i, g + 4 : g + 5, :], 0.0), axis=1, keepdims=True))
        top = jnp.maximum(jnp.maximum(ms[0], ms[1]), jnp.maximum(ms[2], ms[3]))
        es = [jnp.exp2((m - top) * SCALE2) for m in ms]
        num = o_acc[rows, :] * es[0]
        den = ls[0] * es[0]
        for i in (1, 2, 3):
            num += orecv[i, g * 128 : g * 128 + 128, :].astype(F32) * es[i]
            den += ls[i] * es[i]
        att_s[(g % 2) * 128 : (g % 2) * 128 + 128, (g // 2) * 128 : (g // 2) * 128 + 128] = (num / den).astype(BF16)
    for i in (1, 3, 2):
        AT[i].start()
    local[2].wait()
    local[3].wait()
    w(1)
    for i in (1, 2, 3):
        AT[i].wait()
    mixed = RESIDUAL_SCALE * res[...].astype(F32)
    for i in range(4):
        a = att_s[pl.ds(pl.multiple_of(y * 64, 64), 64), :] if i == 0 else attbuf[i]
        mixed += dot(a, ow[pl.ds(pl.multiple_of((y - i + NY) % NY * 256, 256), 256), :])
    xbuf[0:64, :] = layer_norm(mixed, fg_ref[...], fb_ref[...]).astype(BF16)
    YP1.start()
    YM1.start()
    XD[0].start()
    w(2)
    YP1.wait()
    YP2.start()
    XD[1].start()
    YM1.wait()
    YM2.start()
    XD[3].start()
    w(2)
    YP2.wait()
    YM2.wait()
    XD[2].start()
    w(2)
    for i in range(4):
        XD[i].wait()

    u_left = [f for f in u if f in queue[at[0] :]]
    while any(f in queue[at[0] :] for f in u_left):
        w(1)
    for i in order:
        U.have(i)

    def up_tile(i, _):
        cols = pl.ds(pl.multiple_of(i * 256, 256), 256)
        h = jnp.maximum(dot(xbuf[...], upbuf[:, cols]), 0.0)
        hid[:, cols] = (h * h).astype(BF16)
        return 0

    lax.fori_loop(0, 4, up_tile, 0)

    def combine(j, zs):
        DD[j].wait()
        cols = pl.ds(pl.multiple_of(zs * 256, 256), 256)
        both = pown[j % 2] + precv[j].astype(F32)
        fin[:, cols] = both[0:64]
        for k in (1, 2, 3):
            ysend[j, k] = both[k * 64 : k * 64 + 64].astype(BF16)
        for k in (1, 3, 2):
            RS[j][k - 1].start()

    need = {0: d.index(d[5]) + 1, 1: 6, 2: 6, 3: 9, 4: 9, 5: 12, 6: 12, 7: 15}
    done_d = [len([f for f in d if f not in queue[at[0] :]])]
    need[0] = 3
    for j, dz in enumerate(order):
        while done_d[0] < need[j]:
            d[done_d[0]]()
            done_d[0] += 1
        D.have(dz)
        zs = zat(dz)
        part = dot(hid[...], dnbuf[pl.ds(pl.multiple_of(zs * 256, 256), 256), :], ((1,), (1,)))
        pown[j % 2] = part[0:256]
        psend[j] = part[256:512].astype(BF16)
        DD[j].start()
        if j > 0:
            combine(j - 1, zat(order[j - 1]))
    combine(7, zat(4))

    for j, dz in enumerate(order):
        cols = pl.ds(pl.multiple_of(zat(dz) * 256, 256), 256)
        for k in (1, 2, 3):
            RS[j][k - 1].wait()
        fin[:, cols] = fin[:, cols] + (yrecv[j, 1].astype(F32) + yrecv[j, 2].astype(F32) + yrecv[j, 3].astype(F32))
    summed = RESIDUAL_SCALE * xbuf[0:64, :].astype(F32) + fin[...]
    out_ref[...] = layer_norm(summed, sg_ref[...], sb_ref[...]).astype(BF16)
    for t in pool.all:
        t.drain()


def per_device(
    queries, keys, values, residual, query_gain, key_gain, out_weight, first_gain, first_bias, up_weight, down_weight,
    second_gain, second_bias,
):
    cos, sin = rotary_tables()
    sp = lax.axis_index("sp")

    def table(t):
        t = jnp.asarray(t)
        row = jnp.broadcast_to(lax.dynamic_slice_in_dim(t, sp * 4, 4, 0)[:, None, :], (4, GRID_W, 64))
        col = jnp.broadcast_to(t[None, :GRID_W, :], (4, GRID_W, 64))
        return jnp.concatenate([row, col], axis=-1).reshape(256, HEAD_DIM)

    vmem, hbm = pl.BlockSpec(memory_space=pltpu.VMEM), pl.BlockSpec(memory_space=pl.ANY)
    scratch = [
        pltpu.VMEM((KEYS, 256), BF16),
        pltpu.VMEM((2048, 128), BF16),
        pltpu.VMEM((2048, 128), F32),
        pltpu.VMEM((2048, 128), F32),
        pltpu.VMEM((2048, 128), F32),
        pltpu.VMEM((256, KEYS - PASS1), F32),
        pltpu.VMEM((4, 512, 128), BF16),
        pltpu.VMEM((4, 512, 128), BF16),
        pltpu.VMEM((4, 8, 128), F32),
        pltpu.VMEM((4, 8, 128), F32),
        pltpu.VMEM((256, 256), BF16),
        pltpu.VMEM((4, 64, 256), BF16),
        pltpu.VMEM((1024, 2048), BF16),
        pltpu.VMEM((64, 2048), BF16),
        pltpu.VMEM((512, 2048), BF16),
        pltpu.VMEM((2048, W_COLS), BF16),
        pltpu.VMEM((2048, W_COLS), BF16),
        pltpu.VMEM((512, W_COLS), BF16),
        pltpu.VMEM((8, 256, 256), BF16),
        pltpu.VMEM((8, 256, 256), BF16),
        pltpu.VMEM((2, 256, 256), F32),
        pltpu.VMEM((8, 4, 64, 256), BF16),
        pltpu.VMEM((8, 4, 64, 256), BF16),
        pltpu.VMEM((64, 2048), F32),
        pltpu.SemaphoreType.DMA((N_SEMS,)),
        pltpu.SemaphoreType.DMA((N_SEMS,)),
        pltpu.SemaphoreType.DMA((4,)),
    ]
    return pl.pallas_call(
        kernel,
        out_shape=jax.ShapeDtypeStruct((64, 2048), BF16),
        in_specs=[vmem] * 11 + [hbm] * 4,
        out_specs=vmem,
        scratch_shapes=scratch,
        compiler_params=pltpu.CompilerParams(collective_id=0, has_side_effects=True, vmem_limit_bytes=62 * 1024 * 1024),
        name="layer",
    )(
        queries, keys, values, table(cos), table(sin), query_gain[None], key_gain[None], first_gain[None], first_bias[None],
        second_gain[None], second_bias[None], residual, out_weight, up_weight, down_weight,
    )


def solution(mesh):
    in_specs = (
        P("sp", "tp"), P("sp", "tp"), P("sp", "tp"), P(("sp", "tp"), None), P(), P(), P(), P(), P(),
        P("sp", "tp"), P("sp", "tp"), P(), P(),
    )
    return jax.shard_map(per_device, mesh=mesh, in_specs=in_specs, out_specs=P(("sp", "tp"), None), check_vma=False)
```

```python
import functools

import jax
import jax.numpy as jnp
import numpy as np
from jax import lax
from jax.experimental import pallas as pl
from jax.experimental.pallas import tpu as pltpu
from jax.sharding import PartitionSpec as P

MESH = pl.DeviceIdType.MESH
HEAD_DIM = 128
GRID_W = 64
RESIDUAL_SCALE = 2.0**0.25
LAYER_EPS = 1e-05
HEAD_EPS = 1e-06
ROTARY_BASE = 10000.0
NZ, NX, NC, NY = 8, 4, 2, 4
SCALE2 = float(np.log2(np.e) * HEAD_DIM**-0.5)
AW = 640
W_COLS = 1024
PASS1 = 3 * 512
KEYS = 4096
F32, BF16 = jnp.float32, jnp.bfloat16


def rotary_tables():
    inverse = (np.float32(ROTARY_BASE) ** (-np.arange(32, dtype=np.float32) / np.float32(32))).astype(np.float32)
    ang = np.arange(256, dtype=np.float32)[:, None] * inverse
    sign = np.tile(np.array([-1.0, 1.0], np.float32), 32)
    cos = np.repeat(np.cos(ang), 2, axis=1).astype(np.float32)
    sin = np.repeat(np.sin(ang), 2, axis=1).astype(np.float32) * sign
    return cos, sin


class Copy:
    def __init__(self, pool, src, dst, land, dev):
        self.n = pool.take()
        self.pool, self.src, self.dst, self.land, self.dev = pool, src, dst, land, dev

    def start(self):
        self._make(self.src(), self.dst()).start()

    def wait(self):
        here = self.land()
        self._make(here, here).wait_recv()

    def drain(self):
        src = self.src()
        self._make(src, self.dst()).wait_send()

    def _make(self, src, dst):
        return pltpu.make_async_remote_copy(
            src_ref=src, dst_ref=dst, send_sem=self.pool.ssem.at[self.n], recv_sem=self.pool.rsem.at[self.n],
            device_id=self.dev, device_id_type=MESH,
        )


class Phases:
    def __init__(self):
        self.scope = None

    def __call__(self, name):
        if self.scope is not None:
            self.scope.__exit__(None, None, None)
        self.scope = jax.named_scope(name) if name else None
        if name:
            self.scope.__enter__()


class Pool:
    def __init__(self, ssem, rsem, size):
        self.ssem, self.rsem, self.size, self.n, self.all = ssem, rsem, size, 0, []

    def take(self):
        self.n += 1
        assert self.n <= self.size
        return self.n - 1

    def copy(self, src, dst, land, dev):
        c = Copy(self, src, dst, land, dev)
        self.all.append(c)
        return c


N_SEMS = 240


def layer_norm(summed, gain, bias):
    centred = summed - jnp.mean(summed, axis=-1, keepdims=True)
    variance = jnp.mean(centred * centred, axis=-1, keepdims=True)
    return centred * lax.rsqrt(variance + LAYER_EPS) * gain + bias


def norm_rotate(x, gain, cos, sin):
    x = x.astype(F32)
    x = x * lax.rsqrt(jnp.mean(x * x, axis=-1, keepdims=True) + HEAD_EPS) * gain
    even = lax.broadcasted_iota(jnp.int32, x.shape, 1) % 2 == 0
    swapped = jnp.where(even, pltpu.roll(x, HEAD_DIM - 1, 1), pltpu.roll(x, 1, 1))
    return (x * cos + swapped * sin).astype(BF16)


def eye128():
    return lax.broadcasted_iota(jnp.int32, (128, 128), 0) == lax.broadcasted_iota(jnp.int32, (128, 128), 1)


def dot(a, b, dims=((1,), (0,))):
    return lax.dot_general(a, b, (dims, ((), ())), preferred_element_type=F32)


def kernel(
    q_ref, k_ref, v_ref, cosr_ref, cosc_ref, sinr_ref, sinc_ref, qg_ref, kg_ref, fg_ref, fb_ref, sg_ref, sb_ref,
    res_hbm, ow_hbm, up_hbm, dn_hbm,
    out_ref,
    kvbuf, qbuf, o_acc, m_acc, l_acc, s_scr, osend, orecv, stsend, strecv, att_s, attbuf, ow, res, xbuf,
    upbuf, dnbuf, hid, psend, precv, pown, ysend, yrecv, fin,
    ssem, rsem, lsem,
):
    sp, y = lax.axis_index("sp"), lax.axis_index("tp")
    z, x, c = sp // 8, (sp // 2) % 4, sp % 2
    pool = Pool(ssem, rsem, N_SEMS)
    phase = Phases()
    phase("p_prep")

    def dev(dz=0, dx=0, dy=0, flip=False):
        zz, xx, yy = (z + dz + NZ) % NZ, (x + dx + NX) % NX, (y + dy + NY) % NY
        cc = 1 - c if flip else c
        return (zz * 8 + xx * 2 + cc, yy)

    def zat(d):
        return (z + d + NZ) % NZ

    def xat(d):
        return (x + d + NX) % NX

    barrier = pltpu.get_barrier_semaphore()
    partners = [dict(dz=1), dict(dz=-1), dict(dx=1), dict(dx=-1), dict(dx=2), dict(dy=1), dict(dy=-1), dict(dy=2), dict(flip=True)]
    for p in partners:
        pl.semaphore_signal(barrier, inc=1, device_id=dev(**p), device_id_type=MESH)

    def block(zs, xs):
        return pl.multiple_of(zs * 256 + xs * 64, 64)

    mine = pl.multiple_of(c * W_COLS, W_COLS)
    other = pl.multiple_of((1 - c) * W_COLS, W_COLS)
    my_rows = pl.ds(pl.multiple_of(block(z, x) + c * 32, 32), 32)
    partner_rows = pl.ds(pl.multiple_of(block(z, x) + (1 - c) * 32, 32), 32)
    local = [
        pltpu.make_async_copy(up_hbm.at[:, pl.ds(mine, W_COLS)], upbuf.at[my_rows, :], lsem.at[0]),
        pltpu.make_async_copy(dn_hbm.at[:, pl.ds(mine, W_COLS)], dnbuf.at[my_rows, :], lsem.at[1]),
        pltpu.make_async_copy(ow_hbm, ow, lsem.at[2]),
        pltpu.make_async_copy(res_hbm, res, lsem.at[3]),
    ]
    for l in local:
        l.start()

    def angles(rows, cols):
        cols = cols[...]
        parts = [jnp.broadcast_to(rows[pl.ds(sp * 4 + i, 1), :], (GRID_W, HEAD_DIM)) + cols for i in range(4)]
        return jnp.concatenate(parts, axis=0)

    cos, sin = angles(cosr_ref, cosc_ref), angles(sinr_ref, sinc_ref)
    kvbuf[0:256, 0:128] = norm_rotate(k_ref[...], kg_ref[...], cos, sin)
    kvbuf[0:256, 128:256] = v_ref[...]
    qbuf[0:256, :] = norm_rotate(q_ref[:, 0:128], qg_ref[...], cos, sin)
    qbuf[256:512, :] = norm_rotate(q_ref[:, 128:256], qg_ref[...], cos, sin)

    def same(ref, rows, cols, land_rows, device):
        view = lambda: ref.at[pl.ds(*rows), pl.ds(*cols)]
        return pool.copy(view, view, lambda: ref.at[pl.ds(*land_rows), pl.ds(*cols)], device)

    flip = dev(flip=True)
    KP, KM, KD = {}, {}, {}

    def ring(src, dst, lo, device):
        view = lambda slot: kvbuf.at[pl.ds(slot * 512 + lo, 128), :]
        return pool.copy(lambda: view(src), lambda: view(dst), lambda: view(dst), device)

    for s in range(1, 5):
        for h in range(2):
            if s < 4 or h == 0:
                KP[s, h] = ring(0 if s == 1 else 2 * s - 3, 2 * s - 1, h * 128, dev(dz=1))
            if s < 4 or h == 1:
                KM[s, h] = ring(0 if s == 1 else 2 * s - 2, 2 * s if s < 4 else 7, h * 128, dev(dz=-1))
    for j in range(8):
        KD[j] = pool.copy(
            lambda j=j: kvbuf.at[pl.ds(j * 512, 256), :],
            lambda j=j: kvbuf.at[pl.ds(j * 512 + 256, 256), :],
            lambda j=j: kvbuf.at[pl.ds(j * 512 + 256, 256), :], flip)
    QS, OS, ST, AT = {}, {}, {}, {}
    for d in range(1, 4):
        QS[d] = pool.copy(
            lambda: qbuf.at[pl.ds(0, 512), :], lambda d=d: qbuf.at[pl.ds(d * 512, 512), :],
            lambda d=d: qbuf.at[pl.ds(d * 512, 512), :], dev(dx=d))
        OS[d] = pool.copy(lambda d=d: osend.at[d], lambda d=d: orecv.at[d], lambda d=d: orecv.at[d], dev(dx=-d))
        ST[d] = pool.copy(lambda d=d: stsend.at[d], lambda d=d: strecv.at[d], lambda d=d: strecv.at[d], dev(dx=-d))
        AT[d] = pool.copy(
            lambda d=d: att_s.at[pl.ds(pl.multiple_of((y + d) % NY * 64, 64), 64), :],
            lambda d=d: attbuf.at[d], lambda d=d: attbuf.at[d], dev(dy=d))
    def rows_of(ref, lo, n):
        return lambda: ref.at[pl.ds(lo, n), :]

    YP1 = pool.copy(rows_of(xbuf, 0, 64), rows_of(xbuf, 64, 64), rows_of(xbuf, 64, 64), dev(dy=1))
    YM1 = pool.copy(rows_of(xbuf, 0, 64), rows_of(xbuf, 192, 64), rows_of(xbuf, 192, 64), dev(dy=-1))
    YP2 = pool.copy(rows_of(xbuf, 64, 32), rows_of(xbuf, 128, 32), rows_of(xbuf, 128, 32), dev(dy=1))
    YM2 = pool.copy(rows_of(xbuf, 224, 32), rows_of(xbuf, 160, 32), rows_of(xbuf, 160, 32), dev(dy=-1))
    XD = [pool.copy(rows_of(xbuf, j * 64, 64), rows_of(xbuf, 256 + j * 64, 64), rows_of(xbuf, 256 + j * 64, 64), flip) for j in range(4)]

    def exchange(hbm, buf):
        return pool.copy(
            lambda: hbm.at[:, pl.ds(other, W_COLS)], lambda: buf.at[my_rows, :], lambda: buf.at[partner_rows, :], flip)

    WX = {"u": exchange(up_hbm, upbuf), "d": exchange(dn_hbm, dnbuf)}
    order = [0, -1, 1, -2, 2, -3, 3, 4]

    xr = [0, -1, 1, 2]

    class Gather:
        def __init__(self, buf):
            a, b = (0, AW), (AW, W_COLS - AW)
            up, down, right, left = dev(dz=1), dev(dz=-1), dev(dx=1), dev(dx=-1)
            self.AP, self.AM, self.BP, self.BM = {}, {}, {}, {}
            for s in range(1, 5):
                n, h = (64, 0) if s < 4 else (32, 32)
                self.AP[s] = same(buf, (block(zat(1 - s), x), n), a, (block(zat(-s), x), n), up)
                self.AM[s] = same(buf, (block(zat(s - 1), x) + h, n), a, (block(zat(s), x) + h, n), down)
                for i, r in enumerate(xr):
                    if s < 4 or i < 2:
                        self.BP[s, i] = same(buf, (block(zat(1 - s), xat(r)), 64), b, (block(zat(-s), xat(r)), 64), up)
                    if s < 4 or i >= 2:
                        self.BM[s, i] = same(buf, (block(zat(s - 1), xat(r)), 64), b, (block(zat(s), xat(r)), 64), down)
            self.ax = {d: self.spread(buf, zat(d), a, right, left) for d in order}
            self.bx = self.spread(buf, z, b, right, left)

        def spread(self, buf, zs, cols, right, left):
            return (
                same(buf, (block(zs, x), 64), cols, (block(zs, xat(-1)), 64), right),
                same(buf, (block(zs, x), 64), cols, (block(zs, xat(1)), 64), left),
                same(buf, (block(zs, xat(-1)), 32), cols, (block(zs, xat(-2)), 32), right),
                same(buf, (block(zs, xat(1)) + 32, 32), cols, (block(zs, xat(2)) + 32, 32), left),
            )

        def begin(self):
            for t in (self.bx[0], self.bx[1], self.AP[1], self.AM[1], self.BP[1, 0], self.BM[1, 0], self.ax[0][0], self.ax[0][1]):
                t.start()

        def pass_on(self, four):
            four[0].wait()
            four[2].start()
            four[1].wait()
            four[3].start()

        def first_x(self):
            self.pass_on(self.bx)
            for i in (1, 2):
                self.BP[1, i].start()
                self.BM[1, i].start()
            self.pass_on(self.ax[0])

        def row(self):
            self.bx[2].wait()
            self.bx[3].wait()
            self.BP[1, 3].start()
            self.BM[1, 3].start()

        def a_step(self, s):
            self.AP[s].wait()
            if s < 4:
                self.AP[s + 1].start()
            self.AM[s].wait()
            if s < 4:
                self.AM[s + 1].start()
            for d in (-s, s) if s < 4 else (4,):
                self.ax[d][0].start()
                self.ax[d][1].start()

        def b_step(self, s, i):
            for chain in (self.BP, self.BM):
                if (s, i) in chain:
                    chain[s, i].wait()
                    if (s + 1, i) in chain:
                        chain[s + 1, i].start()

        def x_step(self, s):
            for d in (-s, s) if s < 4 else (4,):
                self.pass_on(self.ax[d])

        def have(self, d):
            self.ax[d][2].wait()
            self.ax[d][3].wait()

        def groups(self):
            out = [[self.begin], [self.first_x, self.row]]
            for s in range(1, 5):
                b = [functools.partial(self.b_step, s, i) for i in range(4)]
                out.append([functools.partial(self.a_step, s), b[0], b[1], functools.partial(self.x_step, s), b[2], b[3]])
            return out

    U, D = Gather(upbuf), Gather(dnbuf)
    DD = [pool.copy(lambda j=j: psend.at[j], lambda j=j: precv.at[j], lambda j=j: precv.at[j], flip) for j in range(8)]
    RS = [
        [pool.copy(lambda j=j, k=k: ysend.at[j, k], lambda j=j, k=k: yrecv.at[j, k], lambda j=j, k=k: yrecv.at[j, k], dev(dy=-k)) for k in (1, 2, 3)]
        for j in range(8)
    ]

    ug, dg = U.groups(), D.groups()
    u, d = sum(ug, []), sum(dg, [])
    names = {id(e): t + str(i) + "_" + str(k) for t, gs in (("u", ug), ("d", dg)) for i, g in enumerate(gs) for k, e in enumerate(g)}

    def run(e):
        with jax.named_scope(names.get(id(e), "step")):
            e()

    def first(g):
        return g[:3]

    def second(g):
        return g[4:]

    def across(g):
        return g[3:4]

    queue = ug[0] + ug[1] + dg[0] + first(ug[2]) + second(ug[2]) + dg[1] + across(ug[2])
    for s in (2, 3, 4):
        queue += first(ug[s + 1]) + second(ug[s + 1])
        if s > 2:
            queue += across(dg[s - 1])
        queue += first(dg[s]) + second(dg[s]) + across(ug[s + 1])
    queue += first(dg[5]) + second(dg[5]) + across(dg[4]) + across(dg[5])
    d = [e for e in queue if e in d]
    at = [0]

    def w(n):
        for e in queue[at[0] : at[0] + n]:
            run(e)
        at[0] += n

    phase("p_barrier")
    pl.semaphore_wait(barrier, len(partners))
    for h in range(2):
        KP[1, h].start()
        KM[1, h].start()
    KD[0].start()
    for i in (1, 3, 2):
        QS[i].start()
    WX["u"].start()
    WX["d"].start()
    phase("p_wx")
    local[0].wait()
    WX["u"].wait()
    w(1)
    local[1].wait()
    WX["d"].wait()
    phase("p_kv1")
    def kv_step(s):
        for h in range(2):
            for chain in (KP, KM):
                if (s, h) in chain:
                    chain[s, h].wait()
                    if (s + 1, h) in chain:
                        chain[s + 1, h].start()
        if s < 4:
            KD[2 * s - 1].start()
            KD[2 * s].start()
        else:
            KD[7].start()

    kv_step(1)
    for i in range(3):
        KD[i].wait()
    w(2)
    phase("p_qwait")
    for i in (1, 2, 3):
        QS[i].wait()

    def scores(row, lo, hi):
        q = qbuf[pl.ds(row, 256), :]
        best = None
        for at_key in range(lo, hi, 512):
            part = dot(q, kvbuf[pl.ds(at_key, 512), 0:128], ((1,), (1,)))
            s_scr[:, pl.ds(at_key - lo, 512)] = part
            for g in range(0, 512, 128):
                best = part[:, g : g + 128] if best is None else jnp.maximum(best, part[:, g : g + 128])
        return jnp.max(best, axis=1, keepdims=True)

    def weigh(m, lo, hi):
        total, out = None, None
        for at_key in range(lo, hi, 512):
            p = jnp.exp2((s_scr[:, pl.ds(at_key - lo, 512)] - m) * SCALE2)
            for g in range(0, 512, 128):
                total = p[:, g : g + 128] if total is None else total + p[:, g : g + 128]
            o = dot(p.astype(BF16), kvbuf[pl.ds(at_key, 512), 128:256])
            out = o if out is None else out + o
        return jnp.sum(total, axis=1, keepdims=True), out

    def events_at(i, table):
        for step, fns in table.items():
            @pl.when(i == step)
            def _(fns=fns):
                for f in fns:
                    run(f)

    def pass1(i, _):
        row = pl.multiple_of((i + 2) % 8 * 256, 256)
        m = scores(row, 0, PASS1)
        l, o = weigh(m, 0, PASS1)
        o_acc[pl.ds(row, 256), :] = o
        m_acc[pl.ds(row, 256), :] = jnp.broadcast_to(m, (256, 128))
        l_acc[pl.ds(row, 256), :] = jnp.broadcast_to(l, (256, 128))
        events_at(i, ev1)
        return 0

    def grab(n):
        got = queue[at[0] : at[0] + n]
        at[0] += n
        return got

    ev1 = {
        0: [lambda: kv_step(2)], 1: grab(1), 2: grab(3), 3: [lambda: kv_step(3)], 4: grab(4), 5: grab(1), 6: [lambda: kv_step(4)], 7: grab(3),
    }
    phase("p_pass1")
    lax.fori_loop(0, 8, pass1, 0)
    phase("p_kdwait")
    for i in range(3, 8):
        KD[i].wait()

    def send_o(d):
        eye = eye128()
        for g in range(4):
            rows = pl.ds(d * 512 + g * 128, 128)
            stsend[d, g : g + 1, :] = jnp.sum(jnp.where(eye, m_acc[rows, :], 0.0), axis=0, keepdims=True)
            stsend[d, g + 4 : g + 5, :] = jnp.sum(jnp.where(eye, l_acc[rows, :], 0.0), axis=0, keepdims=True)
        OS[d].start()
        ST[d].start()

    def pass2(i, _):
        row = pl.multiple_of((i + 2) % 8 * 256, 256)
        m_old = m_acc[pl.ds(row, 256), 0:1]
        m = jnp.maximum(scores(row, PASS1, KEYS), m_old)
        alpha = jnp.exp2((m_old - m) * SCALE2)
        l, o = weigh(m, PASS1, KEYS)
        o = o_acc[pl.ds(row, 256), :] * alpha + o
        l = l_acc[pl.ds(row, 256), 0:1] * alpha + l
        o_acc[pl.ds(row, 256), :] = o
        m_acc[pl.ds(row, 256), :] = jnp.broadcast_to(m, (256, 128))
        l_acc[pl.ds(row, 256), :] = jnp.broadcast_to(l, (256, 128))
        osend[row // 512, pl.ds(pl.multiple_of(row % 512, 256), 256), :] = o.astype(BF16)
        events_at(i, ev2)
        return 0

    ev2 = {
        0: grab(2), 1: [lambda: send_o(1)] + grab(3), 2: grab(3), 3: [lambda: send_o(2)] + grab(3), 4: grab(3), 5: [lambda: send_o(3)] + grab(3),
        6: grab(3), 7: grab(3),
    }
    phase("p_pass2")
    lax.fori_loop(0, 8, pass2, 0)

    phase("p_owait")
    for i in (1, 2, 3):
        ST[i].wait()
    for i in (1, 2, 3):
        OS[i].wait()
    phase("p_combine")
    eye = eye128()
    for g in range(4):
        rows = pl.ds(g * 128, 128)
        ms, ls = [m_acc[rows, 0:1]], [l_acc[rows, 0:1]]
        for i in (1, 2, 3):
            ms.append(jnp.sum(jnp.where(eye, strecv[i, g : g + 1, :], 0.0), axis=1, keepdims=True))
            ls.append(jnp.sum(jnp.where(eye, strecv[i, g + 4 : g + 5, :], 0.0), axis=1, keepdims=True))
        top = jnp.maximum(jnp.maximum(ms[0], ms[1]), jnp.maximum(ms[2], ms[3]))
        es = [jnp.exp2((m - top) * SCALE2) for m in ms]
        num = o_acc[rows, :] * es[0]
        den = ls[0] * es[0]
        for i in (1, 2, 3):
            num += orecv[i, g * 128 : g * 128 + 128, :].astype(F32) * es[i]
            den += ls[i] * es[i]
        att_s[(g % 2) * 128 : (g % 2) * 128 + 128, (g // 2) * 128 : (g // 2) * 128 + 128] = (num / den).astype(BF16)
    phase("p_att")
    for i in (1, 3, 2):
        AT[i].start()
    local[2].wait()
    local[3].wait()
    w(3)
    for i in (1, 2, 3):
        AT[i].wait()
    phase("p_mixed")
    mixed = RESIDUAL_SCALE * res[...].astype(F32)
    for i in range(4):
        a = att_s[pl.ds(pl.multiple_of(y * 64, 64), 64), :] if i == 0 else attbuf[i]
        mixed += dot(a, ow[pl.ds(pl.multiple_of((y - i + NY) % NY * 256, 256), 256), :])
    xbuf[0:64, :] = layer_norm(mixed, fg_ref[...], fb_ref[...]).astype(BF16)
    phase("p_yag")
    YP1.start()
    YM1.start()
    XD[0].start()
    w(3)
    YP1.wait()
    YP2.start()
    XD[1].start()
    YM1.wait()
    YM2.start()
    XD[3].start()
    w(3)
    YP2.wait()
    YM2.wait()
    XD[2].start()
    w(3)
    for i in range(4):
        XD[i].wait()

    phase("p_uwait")
    while any(f in u for f in queue[at[0] :]):
        w(1)
    for i in order:
        U.have(i)

    def up_tile(i, _):
        cols = pl.ds(pl.multiple_of(i * 256, 256), 256)
        h = jnp.maximum(dot(xbuf[...], upbuf[:, cols]), 0.0)
        hid[:, cols] = (h * h).astype(BF16)
        return 0

    phase("p_up")
    lax.fori_loop(0, 4, up_tile, 0)

    def combine(j, zs):
        DD[j].wait()
        cols = pl.ds(pl.multiple_of(zs * 256, 256), 256)
        both = pown[j % 2] + precv[j].astype(F32)
        fin[:, cols] = both[0:64]
        for k in (1, 2, 3):
            ysend[j, k] = both[k * 64 : k * 64 + 64].astype(BF16)
        for k in (1, 3, 2):
            RS[j][k - 1].start()

    phase("p_down")
    need = {dz: max(i for i, e in enumerate(d) if any(e in g for g in dg[: abs(dz) + 2])) + 1 for dz in order}
    done_d = [len([f for f in d if f not in queue[at[0] :]])]
    for j, dz in enumerate(order):
        while done_d[0] < need[dz]:
            run(d[done_d[0]])
            done_d[0] += 1
        D.have(dz)
        zs = zat(dz)
        part = dot(hid[...], dnbuf[pl.ds(pl.multiple_of(zs * 256, 256), 256), :], ((1,), (1,)))
        pown[j % 2] = part[0:256]
        psend[j] = part[256:512].astype(BF16)
        DD[j].start()
        if j > 0:
            combine(j - 1, zat(order[j - 1]))
    combine(7, zat(4))

    phase("p_last")
    for j, dz in enumerate(order):
        cols = pl.ds(pl.multiple_of(zat(dz) * 256, 256), 256)
        for k in (1, 2, 3):
            RS[j][k - 1].wait()
        fin[:, cols] = fin[:, cols] + (yrecv[j, 1].astype(F32) + yrecv[j, 2].astype(F32) + yrecv[j, 3].astype(F32))
    summed = RESIDUAL_SCALE * xbuf[0:64, :].astype(F32) + fin[...]
    out_ref[...] = layer_norm(summed, sg_ref[...], sb_ref[...]).astype(BF16)
    phase("p_drain")
    for t in pool.all:
        t.drain()
    phase(None)


def per_device(
    queries, keys, values, residual, query_gain, key_gain, out_weight, first_gain, first_bias, up_weight, down_weight,
    second_gain, second_bias,
):
    cos, sin = rotary_tables()
    zero = np.zeros((256, 64), np.float32)

    def table(t):
        return jnp.asarray(np.concatenate([t, zero], 1)), jnp.asarray(np.concatenate([zero, t], 1)[:GRID_W])

    vmem, hbm = pl.BlockSpec(memory_space=pltpu.VMEM), pl.BlockSpec(memory_space=pl.ANY)
    scratch = [
        pltpu.VMEM((KEYS, 256), BF16),
        pltpu.VMEM((2048, 128), BF16),
        pltpu.VMEM((2048, 128), F32),
        pltpu.VMEM((2048, 128), F32),
        pltpu.VMEM((2048, 128), F32),
        pltpu.VMEM((256, KEYS - PASS1), F32),
        pltpu.VMEM((4, 512, 128), BF16),
        pltpu.VMEM((4, 512, 128), BF16),
        pltpu.VMEM((4, 8, 128), F32),
        pltpu.VMEM((4, 8, 128), F32),
        pltpu.VMEM((256, 256), BF16),
        pltpu.VMEM((4, 64, 256), BF16),
        pltpu.VMEM((1024, 2048), BF16),
        pltpu.VMEM((64, 2048), BF16),
        pltpu.VMEM((512, 2048), BF16),
        pltpu.VMEM((2048, W_COLS), BF16),
        pltpu.VMEM((2048, W_COLS), BF16),
        pltpu.VMEM((512, W_COLS), BF16),
        pltpu.VMEM((8, 256, 256), BF16),
        pltpu.VMEM((8, 256, 256), BF16),
        pltpu.VMEM((2, 256, 256), F32),
        pltpu.VMEM((8, 4, 64, 256), BF16),
        pltpu.VMEM((8, 4, 64, 256), BF16),
        pltpu.VMEM((64, 2048), F32),
        pltpu.SemaphoreType.DMA((N_SEMS,)),
        pltpu.SemaphoreType.DMA((N_SEMS,)),
        pltpu.SemaphoreType.DMA((4,)),
    ]
    return pl.pallas_call(
        kernel,
        out_shape=jax.ShapeDtypeStruct((64, 2048), BF16),
        in_specs=[vmem] * 13 + [hbm] * 4,
        out_specs=vmem,
        scratch_shapes=scratch,
        compiler_params=pltpu.CompilerParams(collective_id=0, has_side_effects=True, vmem_limit_bytes=62 * 1024 * 1024),
        name="layer",
    )(
        queries, keys, values, *table(cos), *table(sin), query_gain[None], key_gain[None], first_gain[None], first_bias[None],
        second_gain[None], second_bias[None], residual, out_weight, up_weight, down_weight,
    )


def solution(mesh):
    in_specs = (
        P("sp", "tp"), P("sp", "tp"), P("sp", "tp"), P(("sp", "tp"), None), P(), P(), P(), P(), P(),
        P("sp", "tp"), P("sp", "tp"), P(), P(),
    )
    return jax.shard_map(per_device, mesh=mesh, in_specs=in_specs, out_specs=P(("sp", "tp"), None), check_vma=False)
```

```python
import functools

import jax
import jax.numpy as jnp
import numpy as np
from jax import lax
from jax.experimental import pallas as pl
from jax.experimental.pallas import tpu as pltpu
from jax.sharding import PartitionSpec as P

MESH = pl.DeviceIdType.MESH
HEAD_DIM = 128
GRID_W = 64
RESIDUAL_SCALE = 2.0**0.25
LAYER_EPS = 1e-05
HEAD_EPS = 1e-06
ROTARY_BASE = 10000.0
NZ, NX, NC, NY = 8, 4, 2, 4
SCALE2 = float(np.log2(np.e) * HEAD_DIM**-0.5)
AW = 640
W_COLS = 1024
PASS1, PASS2 = 3 * 512, 5 * 512
KEYS = 4096
F32, BF16 = jnp.float32, jnp.bfloat16


def rotary_tables():
    inverse = (np.float32(ROTARY_BASE) ** (-np.arange(32, dtype=np.float32) / np.float32(32))).astype(np.float32)
    ang = np.arange(256, dtype=np.float32)[:, None] * inverse
    sign = np.tile(np.array([-1.0, 1.0], np.float32), 32)
    cos = np.repeat(np.cos(ang), 2, axis=1).astype(np.float32)
    sin = np.repeat(np.sin(ang), 2, axis=1).astype(np.float32) * sign
    return cos, sin


class Copy:
    def __init__(self, pool, src, dst, land, dev):
        self.n = pool.take()
        self.pool, self.src, self.dst, self.land, self.dev = pool, src, dst, land, dev

    def start(self):
        self._make(self.src(), self.dst()).start()

    def wait(self):
        here = self.land()
        self._make(here, here).wait_recv()

    def drain(self):
        src = self.src()
        self._make(src, self.dst()).wait_send()

    def _make(self, src, dst):
        return pltpu.make_async_remote_copy(
            src_ref=src, dst_ref=dst, send_sem=self.pool.ssem.at[self.n], recv_sem=self.pool.rsem.at[self.n],
            device_id=self.dev, device_id_type=MESH,
        )


class Phases:
    def __init__(self):
        self.scope = None

    def __call__(self, name):
        if self.scope is not None:
            self.scope.__exit__(None, None, None)
        self.scope = jax.named_scope(name) if name else None
        if name:
            self.scope.__enter__()


class Pool:
    def __init__(self, ssem, rsem, size):
        self.ssem, self.rsem, self.size, self.n, self.all = ssem, rsem, size, 0, []

    def take(self):
        self.n += 1
        assert self.n <= self.size
        return self.n - 1

    def copy(self, src, dst, land, dev):
        c = Copy(self, src, dst, land, dev)
        self.all.append(c)
        return c


N_SEMS = 264


def layer_norm(summed, gain, bias):
    centred = summed - jnp.mean(summed, axis=-1, keepdims=True)
    variance = jnp.mean(centred * centred, axis=-1, keepdims=True)
    return centred * lax.rsqrt(variance + LAYER_EPS) * gain + bias


def norm_rotate(x, gain, cos, sin):
    x = x.astype(F32)
    x = x * lax.rsqrt(jnp.mean(x * x, axis=-1, keepdims=True) + HEAD_EPS) * gain
    even = lax.broadcasted_iota(jnp.int32, x.shape, 1) % 2 == 0
    swapped = jnp.where(even, pltpu.roll(x, HEAD_DIM - 1, 1), pltpu.roll(x, 1, 1))
    return (x * cos + swapped * sin).astype(BF16)


def dot(a, b, dims=((1,), (0,))):
    return lax.dot_general(a, b, (dims, ((), ())), preferred_element_type=F32)


def kernel(
    q_ref, k_ref, v_ref, cosr_ref, cosc_ref, sinr_ref, sinc_ref, qg_ref, kg_ref, fg_ref, fb_ref, sg_ref, sb_ref,
    res_hbm, ow_hbm, up_hbm, dn_hbm,
    out_ref,
    kbuf, vtbuf, qbuf, o_acc, m_acc, l_acc, s_even, s_odd, osend, orecv, stsend, strecv, att_s, attbuf, ow, res, xbuf,
    upbuf, dnbuf, hid, psend, precv, pown, ysend, yrecv, fin,
    ssem, rsem, lsem,
):
    sp, y = lax.axis_index("sp"), lax.axis_index("tp")
    z, x, c = sp // 8, (sp // 2) % 4, sp % 2
    pool = Pool(ssem, rsem, N_SEMS)
    phase = Phases()
    phase("p_prep")

    def dev(dz=0, dx=0, dy=0, flip=False):
        zz, xx, yy = (z + dz + NZ) % NZ, (x + dx + NX) % NX, (y + dy + NY) % NY
        cc = 1 - c if flip else c
        return (zz * 8 + xx * 2 + cc, yy)

    def zat(d):
        return (z + d + NZ) % NZ

    def xat(d):
        return (x + d + NX) % NX

    barrier = pltpu.get_barrier_semaphore()
    partners = [dict(dz=1), dict(dz=-1), dict(dx=1), dict(dx=-1), dict(dx=2), dict(dy=1), dict(dy=-1), dict(dy=2), dict(flip=True)]
    for p in partners:
        pl.semaphore_signal(barrier, inc=1, device_id=dev(**p), device_id_type=MESH)

    def block(zs, xs):
        return pl.multiple_of(zs * 256 + xs * 64, 64)

    mine = pl.multiple_of(c * W_COLS, W_COLS)
    other = pl.multiple_of((1 - c) * W_COLS, W_COLS)
    my_rows = pl.ds(pl.multiple_of(block(z, x) + c * 32, 32), 32)
    partner_rows = pl.ds(pl.multiple_of(block(z, x) + (1 - c) * 32, 32), 32)
    local = [
        pltpu.make_async_copy(up_hbm.at[:, pl.ds(mine, W_COLS)], upbuf.at[my_rows, :], lsem.at[0]),
        pltpu.make_async_copy(dn_hbm.at[:, pl.ds(mine, W_COLS)], dnbuf.at[my_rows, :], lsem.at[1]),
        pltpu.make_async_copy(ow_hbm, ow, lsem.at[2]),
        pltpu.make_async_copy(res_hbm, res, lsem.at[3]),
    ]
    for l in local:
        l.start()

    def angles(rows, cols):
        cols = cols[...]
        parts = [jnp.broadcast_to(rows[pl.ds(sp * 4 + i, 1), :], (GRID_W, HEAD_DIM)) + cols for i in range(4)]
        return jnp.concatenate(parts, axis=0)

    cos, sin = angles(cosr_ref, cosc_ref), angles(sinr_ref, sinc_ref)
    kbuf[0:256, :] = norm_rotate(k_ref[...], kg_ref[...], cos, sin)
    vtbuf[:, 0:256] = jnp.transpose(v_ref[...].astype(F32)).astype(BF16)
    qbuf[0:256, :] = norm_rotate(q_ref[:, 0:128], qg_ref[...], cos, sin)
    qbuf[256:512, :] = norm_rotate(q_ref[:, 128:256], qg_ref[...], cos, sin)

    def same(ref, rows, cols, land_rows, device):
        view = lambda: ref.at[pl.ds(*rows), pl.ds(*cols)]
        return pool.copy(view, view, lambda: ref.at[pl.ds(*land_rows), pl.ds(*cols)], device)

    flip = dev(flip=True)
    KP, KM, KD = {}, {}, {}

    def place(at_key, h):
        return kbuf.at[pl.ds(at_key, 256), :] if h == 0 else vtbuf.at[:, pl.ds(at_key, 256)]

    def ring(src, dst, h, device):
        return pool.copy(lambda: place(src * 512, h), lambda: place(dst * 512, h), lambda: place(dst * 512, h), device)

    for s in range(1, 5):
        for h in range(2):
            if s < 4 or h == 0:
                KP[s, h] = ring(0 if s == 1 else 2 * s - 3, 2 * s - 1, h, dev(dz=1))
            if s < 4 or h == 1:
                KM[s, h] = ring(0 if s == 1 else 2 * s - 2, 2 * s if s < 4 else 7, h, dev(dz=-1))
    class Both(list):
        def start(self):
            for t in self:
                t.start()

        def wait(self):
            for t in self:
                t.wait()

    def to_other(j, h):
        there = lambda: place(j * 512 + 256, h)
        return pool.copy(lambda: place(j * 512, h), there, there, flip)

    for j in range(8):
        KD[j] = Both(to_other(j, h) for h in range(2))
    QS, OS, ST, AT = {}, {}, {}, {}
    for d in range(1, 4):
        QS[d] = pool.copy(
            lambda: qbuf.at[pl.ds(0, 512), :], lambda d=d: qbuf.at[pl.ds(d * 512, 512), :],
            lambda d=d: qbuf.at[pl.ds(d * 512, 512), :], dev(dx=d))
        for h in range(2):
            OS[d, h] = pool.copy(
                lambda d=d, h=h: osend.at[d, h], lambda d=d, h=h: orecv.at[d, h], lambda d=d, h=h: orecv.at[d, h], dev(dx=-d))
        ST[d] = pool.copy(lambda d=d: stsend.at[d], lambda d=d: strecv.at[d], lambda d=d: strecv.at[d], dev(dx=-d))
        AT[d] = pool.copy(
            lambda d=d: att_s.at[pl.ds(pl.multiple_of((y + d) % NY * 64, 64), 64), :],
            lambda d=d: attbuf.at[d], lambda d=d: attbuf.at[d], dev(dy=d))
    def rows_of(ref, lo, n):
        return lambda: ref.at[pl.ds(lo, n), :]

    YP = [pool.copy(rows_of(xbuf, h, 32), rows_of(xbuf, 128 + h, 32), rows_of(xbuf, 128 + h, 32), dev(dy=1)) for h in (0, 32)]
    YM = [pool.copy(rows_of(xbuf, h, 32), rows_of(xbuf, 384 + h, 32), rows_of(xbuf, 384 + h, 32), dev(dy=-1)) for h in (32, 0)]
    YP2 = pool.copy(rows_of(xbuf, 128, 32), rows_of(xbuf, 256, 32), rows_of(xbuf, 256, 32), dev(dy=1))
    YM2 = pool.copy(rows_of(xbuf, 416, 32), rows_of(xbuf, 288, 32), rows_of(xbuf, 288, 32), dev(dy=-1))
    XD = [pool.copy(rows_of(xbuf, j * 128, 64), rows_of(xbuf, j * 128 + 64, 64), rows_of(xbuf, j * 128 + 64, 64), flip) for j in range(4)]

    def exchange(hbm, buf):
        return pool.copy(
            lambda: hbm.at[:, pl.ds(other, W_COLS)], lambda: buf.at[my_rows, :], lambda: buf.at[partner_rows, :], flip)

    WX = {"u": exchange(up_hbm, upbuf), "d": exchange(dn_hbm, dnbuf)}
    order = [0, -1, 1, -2, 2, -3, 3, 4]

    xr = [0, -1, 1, 2]

    class Gather:
        def __init__(self, buf):
            a, b = (0, AW), (AW, W_COLS - AW)
            up, down, right, left = dev(dz=1), dev(dz=-1), dev(dx=1), dev(dx=-1)
            self.AP, self.AM, self.BP, self.BM = {}, {}, {}, {}
            for s in range(1, 5):
                n, h = (64, 0) if s < 4 else (32, 32)
                self.AP[s] = same(buf, (block(zat(1 - s), x), n), a, (block(zat(-s), x), n), up)
                self.AM[s] = same(buf, (block(zat(s - 1), x) + h, n), a, (block(zat(s), x) + h, n), down)
                for i, r in enumerate(xr):
                    if s < 4 or i < 2:
                        self.BP[s, i] = same(buf, (block(zat(1 - s), xat(r)), 64), b, (block(zat(-s), xat(r)), 64), up)
                    if s < 4 or i >= 2:
                        self.BM[s, i] = same(buf, (block(zat(s - 1), xat(r)), 64), b, (block(zat(s), xat(r)), 64), down)
            self.ax = {d: self.spread(buf, zat(d), a, right, left) for d in order}
            self.bx = self.spread(buf, z, b, right, left)

        def spread(self, buf, zs, cols, right, left):
            return (
                same(buf, (block(zs, x), 64), cols, (block(zs, xat(-1)), 64), right),
                same(buf, (block(zs, x), 64), cols, (block(zs, xat(1)), 64), left),
                same(buf, (block(zs, xat(-1)), 32), cols, (block(zs, xat(-2)), 32), right),
                same(buf, (block(zs, xat(1)) + 32, 32), cols, (block(zs, xat(2)) + 32, 32), left),
            )

        def pass_on(self, four):
            four[0].wait()
            four[2].start()
            four[1].wait()
            four[3].start()

        def a_step(self, s):
            self.AP[s].wait()
            if s < 4:
                self.AP[s + 1].start()
            self.AM[s].wait()
            if s < 4:
                self.AM[s + 1].start()
            for d in (-s, s) if s < 4 else (4,):
                self.ax[d][0].start()
                self.ax[d][1].start()

        def b_step(self, s, i):
            for chain in (self.BP, self.BM):
                if (s, i) in chain:
                    chain[s, i].wait()
                    if (s + 1, i) in chain:
                        chain[s + 1, i].start()

        def x_step(self, s):
            for d in (-s, s) if s < 4 else (4,):
                self.pass_on(self.ax[d])

        def have(self, d):
            self.ax[d][2].wait()
            self.ax[d][3].wait()

        def early(self):
            for t in (self.bx[0], self.bx[1], self.ax[0][0], self.ax[0][1]):
                t.start()

        def early_on(self):
            self.pass_on(self.bx)

        def late(self):
            for t in (self.AP[1], self.AM[1], self.BP[1, 0], self.BM[1, 0]):
                t.start()
            self.bx[2].wait()
            self.bx[3].wait()
            for i in (1, 2, 3):
                self.BP[1, i].start()
                self.BM[1, i].start()

        def own_on(self):
            self.pass_on(self.ax[0])

        def groups(self):
            out = [[self.early], [self.early_on, self.late, self.own_on]]
            for s in range(1, 5):
                b = [functools.partial(self.b_step, s, i) for i in range(4)]
                out.append([functools.partial(self.a_step, s), b[0], b[1], functools.partial(self.x_step, s), b[2], b[3]])
            return out

    U, D = Gather(upbuf), Gather(dnbuf)
    DD = [pool.copy(lambda j=j: psend.at[j], lambda j=j: precv.at[j], lambda j=j: precv.at[j], flip) for j in range(8)]
    RS = [
        [pool.copy(lambda j=j, k=k: ysend.at[j, k], lambda j=j, k=k: yrecv.at[j, k], lambda j=j, k=k: yrecv.at[j, k], dev(dy=-k)) for k in (1, 2, 3)]
        for j in range(8)
    ]

    ug, dg = U.groups(), D.groups()
    u, d = sum(ug, []), sum(dg, [])
    names = {id(e): t + str(i) + "_" + str(k) for t, gs in (("u", ug), ("d", dg)) for i, g in enumerate(gs) for k, e in enumerate(g)}

    def run(e):
        with jax.named_scope(names.get(id(e), "step")):
            e()

    def first(g):
        return g[:3]

    def second(g):
        return g[4:]

    def across(g):
        return g[3:4]

    def step(g):
        return first(g) + second(g)

    queue = ug[0] + dg[0] + ug[1] + dg[1][:1] + dg[1][2:] + step(ug[2])
    queue += across(ug[2]) + dg[1][1:2] + step(ug[3]) + across(ug[3]) + step(ug[4]) + step(dg[2])
    queue += across(ug[4]) + step(ug[5]) + across(dg[2]) + across(ug[5]) + step(dg[3])
    queue += across(dg[3]) + step(dg[4]) + across(dg[4]) + step(dg[5]) + across(dg[5])
    d = [e for e in queue if e in d]
    at = [0]

    def w(n):
        for e in queue[at[0] : at[0] + n]:
            run(e)
        at[0] += n

    phase("p_barrier")
    pl.semaphore_wait(barrier, len(partners))
    for h in range(2):
        KP[1, h].start()
        KM[1, h].start()
    KD[0].start()
    for i in (1, 3, 2):
        QS[i].start()
    WX["u"].start()
    WX["d"].start()
    phase("p_wx")
    local[0].wait()
    WX["u"].wait()
    w(1)
    local[1].wait()
    WX["d"].wait()
    w(1)
    phase("p_kv1")
    def kv_step(s):
        for h in range(2):
            for chain in (KP, KM):
                if (s, h) in chain:
                    chain[s, h].wait()
                    if (s + 1, h) in chain:
                        chain[s + 1, h].start()
        if s < 4:
            KD[2 * s - 1].start()
            KD[2 * s].start()
        else:
            KD[7].start()

    kv_step(1)
    for i in range(3):
        KD[i].wait()
    phase("p_qwait")

    def tile_scores(t, at_key, dst, lo, best):
        q = qbuf[pl.ds(pl.multiple_of(t * 256, 256), 256), :]
        part = dot(kbuf[pl.ds(at_key, 512), :], q, ((1,), (1,)))
        dst[pl.ds(at_key - lo, 512), :] = part
        top = jnp.max(part.reshape(64, 8, 256), axis=0)
        return top if best is None else jnp.maximum(best, top)

    def stage(t_next, t, src, dst, m, lo, hi):
        best, total, out = None, None, None
        for at_key in range(lo, hi, 512):
            best = tile_scores(t_next, at_key, dst, lo, best)
            p = jnp.exp2((src[pl.ds(at_key - lo, 512), :] - m) * SCALE2)
            part = jnp.sum(p.reshape(64, 8, 256), axis=0)
            o = dot(vtbuf[:, pl.ds(at_key, 512)], p.astype(BF16))
            total, out = (part, o) if total is None else (total + part, out + o)
        l = jnp.sum(total, axis=0, keepdims=True)
        m_next = jnp.max(best, axis=0, keepdims=True)
        if lo > 0:
            m_old = m_acc[t, 0:1, :]
            alpha = jnp.exp2((m_old - m) * SCALE2)
            out = o_acc[t] * alpha + out
            l = l_acc[t, 0:1, :] * alpha + l
            m_next = jnp.maximum(m_next, m_acc[t_next, 0:1, :])
        if hi == KEYS:
            upper = lax.broadcasted_iota(jnp.int32, (8, 256), 0) < 4
            stsend[t // 2, t % 2] = jnp.where(upper, jnp.broadcast_to(m, (8, 256)), jnp.broadcast_to(l, (8, 256)))
            osend[t // 2, t % 2] = out.astype(BF16)
        o_acc[t] = out
        m_acc[t] = jnp.broadcast_to(m, (8, 256))
        l_acc[t] = jnp.broadcast_to(l, (8, 256))
        return m_next

    def all_tiles(lo, hi, table):
        def slot_of(i):
            return (2 + i * (i + 1) // 2) % 4 if hi == KEYS else i % 4

        best, t = None, 2 * slot_of(0)
        for at_key in range(lo, hi, 512):
            best = tile_scores(t, at_key, s_even, lo, best)
        m = jnp.max(best, axis=0, keepdims=True)
        if lo > 0:
            m = jnp.maximum(m, m_acc[t, 0:1, :])

        def two(i, m):
            t = 2 * slot_of(i)
            m = stage(t + 1, t, s_even, s_odd, m, lo, hi)
            events_at(i, {k // 2: f for k, f in table.items() if k % 2 == 0})
            m = stage(2 * slot_of(i + 1), t + 1, s_odd, s_even, m, lo, hi)
            events_at(i, {k // 2: f for k, f in table.items() if k % 2 == 1})
            return m

        lax.fori_loop(0, 4, two, m)

    def events_at(i, table):
        for step, fns in table.items():
            @pl.when(i == step)
            def _(fns=fns):
                for f in fns:
                    run(f)

    def grab(n):
        got = queue[at[0] : at[0] + n]
        at[0] += n
        return got

    def queries_from(*who):
        return [lambda: [QS[i].wait() for i in who]]

    ev1 = {
        0: queries_from(1, 3) + grab(1), 1: [lambda: kv_step(2)], 2: queries_from(2) + grab(1), 4: grab(1), 5: grab(1), 6: grab(1),
    }
    ev2 = {0: [lambda: kv_step(3)], 7: [lambda: kv_step(4)]}
    phase("p_pass1")
    all_tiles(0, PASS1, ev1)
    phase("p_pass1b")
    for i in (3, 4):
        KD[i].wait()
    all_tiles(PASS1, PASS2, ev2)
    phase("p_kdwait")
    w(5)
    for i in (5, 6, 7):
        KD[i].wait()

    def send_o(d, h):
        def go():
            OS[d, h].start()
            if h == 1:
                ST[d].start()

        return [go]

    ev3 = {2 * i + h: send_o(d, h) for i, d in enumerate((2, 3, 1)) for h in range(2)}
    for k, n in ((1, 1), (3, 1), (5, 3)):
        ev3[k] = ev3[k] + grab(n)
    phase("p_pass2")
    all_tiles(PASS2, KEYS, ev3)

    phase("p_owait")
    w(6)
    for i in (1, 2, 3):
        ST[i].wait()
    for i in (1, 2, 3):
        OS[i, 0].wait()
        OS[i, 1].wait()
    phase("p_combine")
    for h in range(2):
        ms, ls = [m_acc[h, 0:1, :]], [l_acc[h, 0:1, :]]
        for i in (1, 2, 3):
            ms.append(strecv[i, h, 0:1, :])
            ls.append(strecv[i, h, 4:5, :])
        top = jnp.maximum(jnp.maximum(ms[0], ms[1]), jnp.maximum(ms[2], ms[3]))
        es = [jnp.exp2((m - top) * SCALE2) for m in ms]
        num = o_acc[h] * es[0]
        den = ls[0] * es[0]
        for i in (1, 2, 3):
            num += orecv[i, h].astype(F32) * es[i]
            den += ls[i] * es[i]
        att_s[:, h * 128 : h * 128 + 128] = jnp.transpose(num / den).astype(BF16)
    phase("p_att")
    for i in (1, 3, 2):
        AT[i].start()
    local[2].wait()
    local[3].wait()
    w(7)
    phase("q_atwait")
    for i in (1, 2, 3):
        AT[i].wait()
    phase("p_mixed")
    mixed = RESIDUAL_SCALE * res[...].astype(F32)
    for i in range(4):
        a = att_s[pl.ds(pl.multiple_of(y * 64, 64), 64), :] if i == 0 else attbuf[i]
        mixed += dot(a, ow[pl.ds(pl.multiple_of((y - i + NY) % NY * 256, 256), 256), :])
    xbuf[0:64, :] = layer_norm(mixed, fg_ref[...], fb_ref[...]).astype(BF16)
    phase("p_yag")
    for t in (YP[0], YM[0], YP[1], YM[1], XD[0]):
        t.start()
    w(7)
    phase("q_yp1")
    YP[0].wait()
    YP2.start()
    YM[0].wait()
    YM2.start()
    YP[1].wait()
    XD[1].start()
    YM[1].wait()
    XD[3].start()
    w(6)
    assert not any(e in u for e in queue[at[0] :])
    phase("q_uhave")
    for i in order:
        U.have(i)

    def up_rows(lo):
        def tile(i, _):
            cols = pl.ds(pl.multiple_of(i * 256, 256), 256)
            h = jnp.maximum(dot(xbuf[pl.ds(lo, 128), :], upbuf[:, cols]), 0.0)
            hid[pl.ds(lo, 128), cols] = (h * h).astype(BF16)
            return 0

        lax.fori_loop(0, 4, tile, 0)

    phase("q_up0")
    XD[0].wait()
    up_rows(0)
    w(1)
    XD[1].wait()
    up_rows(128)
    w(3)
    XD[3].wait()
    up_rows(384)
    w(2)
    phase("q_yp2")
    YP2.wait()
    YM2.wait()
    XD[2].start()
    phase("q_xd")
    XD[2].wait()
    phase("q_up2")
    up_rows(256)

    def combine(j, zs):
        phase("q_ddwait")
        DD[j].wait()
        phase("q_comb")
        cols = pl.ds(pl.multiple_of(zs * 256, 256), 256)
        both = pown[j % 2] + precv[j].astype(F32)
        fin[:, cols] = both[0:64]
        for k in (1, 2, 3):
            ysend[j, k] = both[k * 64 : k * 64 + 64].astype(BF16)
        for k in (1, 3, 2):
            RS[j][k - 1].start()

    phase("p_down")
    need = {dz: max(i for i, e in enumerate(d) if any(e in g for g in dg[: abs(dz) + 2])) + 1 for dz in order}
    ahead = {0: len(d) - 7, 1: len(d) - 3, 2: len(d) - 1, 3: len(d) - 1}
    done_d = [len([f for f in d if f not in queue[at[0] :]])]
    for j, dz in enumerate(order):
        while done_d[0] < max(need[dz], ahead.get(j, len(d))):
            run(d[done_d[0]])
            done_d[0] += 1
        phase("q_have")
        D.have(dz)
        phase("q_dot")
        zs = zat(dz)
        part = dot(hid[...], dnbuf[pl.ds(pl.multiple_of(zs * 256, 256), 256), :], ((1,), (1,)))
        for i in range(4):
            pown[j % 2, i * 64 : i * 64 + 64, :] = part[i * 128 : i * 128 + 64]
            psend[j, i * 64 : i * 64 + 64, :] = part[i * 128 + 64 : i * 128 + 128].astype(BF16)
        DD[j].start()
        if j > 0:
            combine(j - 1, zat(order[j - 1]))
    combine(7, zat(4))

    phase("p_last")
    for j, dz in enumerate(order):
        cols = pl.ds(pl.multiple_of(zat(dz) * 256, 256), 256)
        phase("q_rswait")
        for k in (1, 2, 3):
            RS[j][k - 1].wait()
        phase("q_fin")
        fin[:, cols] = fin[:, cols] + (yrecv[j, 1].astype(F32) + yrecv[j, 2].astype(F32) + yrecv[j, 3].astype(F32))
    summed = RESIDUAL_SCALE * xbuf[0:64, :].astype(F32) + fin[...]
    out_ref[...] = layer_norm(summed, sg_ref[...], sb_ref[...]).astype(BF16)
    phase("p_drain")
    for t in pool.all:
        t.drain()
    phase(None)


def per_device(
    queries, keys, values, residual, query_gain, key_gain, out_weight, first_gain, first_bias, up_weight, down_weight,
    second_gain, second_bias,
):
    cos, sin = rotary_tables()
    zero = np.zeros((256, 64), np.float32)

    def table(t):
        return jnp.asarray(np.concatenate([t, zero], 1)), jnp.asarray(np.concatenate([zero, t], 1)[:GRID_W])

    vmem, hbm = pl.BlockSpec(memory_space=pltpu.VMEM), pl.BlockSpec(memory_space=pl.ANY)
    scratch = [
        pltpu.VMEM((KEYS, 128), BF16),
        pltpu.VMEM((128, KEYS), BF16),
        pltpu.VMEM((2048, 128), BF16),
        pltpu.VMEM((8, 128, 256), F32),
        pltpu.VMEM((8, 8, 256), F32),
        pltpu.VMEM((8, 8, 256), F32),
        pltpu.VMEM((1536, 256), F32),
        pltpu.VMEM((1536, 256), F32),
        pltpu.VMEM((4, 2, 128, 256), BF16),
        pltpu.VMEM((4, 2, 128, 256), BF16),
        pltpu.VMEM((4, 2, 8, 256), F32),
        pltpu.VMEM((4, 2, 8, 256), F32),
        pltpu.VMEM((256, 256), BF16),
        pltpu.VMEM((4, 64, 256), BF16),
        pltpu.VMEM((1024, 2048), BF16),
        pltpu.VMEM((64, 2048), BF16),
        pltpu.VMEM((512, 2048), BF16),
        pltpu.VMEM((2048, W_COLS), BF16),
        pltpu.VMEM((2048, W_COLS), BF16),
        pltpu.VMEM((512, W_COLS), BF16),
        pltpu.VMEM((8, 256, 256), BF16),
        pltpu.VMEM((8, 256, 256), BF16),
        pltpu.VMEM((2, 256, 256), F32),
        pltpu.VMEM((8, 4, 64, 256), BF16),
        pltpu.VMEM((8, 4, 64, 256), BF16),
        pltpu.VMEM((64, 2048), F32),
        pltpu.SemaphoreType.DMA((N_SEMS,)),
        pltpu.SemaphoreType.DMA((N_SEMS,)),
        pltpu.SemaphoreType.DMA((4,)),
    ]
    return pl.pallas_call(
        kernel,
        out_shape=jax.ShapeDtypeStruct((64, 2048), BF16),
        in_specs=[vmem] * 13 + [hbm] * 4,
        out_specs=vmem,
        scratch_shapes=scratch,
        compiler_params=pltpu.CompilerParams(collective_id=0, has_side_effects=True, vmem_limit_bytes=62 * 1024 * 1024),
        name="layer",
    )(
        queries, keys, values, *table(cos), *table(sin), query_gain[None], key_gain[None], first_gain[None], first_bias[None],
        second_gain[None], second_bias[None], residual, out_weight, up_weight, down_weight,
    )


def solution(mesh):
    in_specs = (
        P("sp", "tp"), P("sp", "tp"), P("sp", "tp"), P(("sp", "tp"), None), P(), P(), P(), P(), P(),
        P("sp", "tp"), P("sp", "tp"), P(), P(),
    )
    return jax.shard_map(per_device, mesh=mesh, in_specs=in_specs, out_specs=P(("sp", "tp"), None), check_vma=False)
```

```python
import functools

import jax
import jax.numpy as jnp
import numpy as np
from jax import lax
from jax.experimental import pallas as pl
from jax.experimental.pallas import tpu as pltpu
from jax.sharding import PartitionSpec as P

MESH = pl.DeviceIdType.MESH
HEAD_DIM = 128
GRID_W = 64
RESIDUAL_SCALE = 2.0**0.25
LAYER_EPS = 1e-05
HEAD_EPS = 1e-06
ROTARY_BASE = 10000.0
NZ, NX, NC, NY = 8, 4, 2, 4
SCALE2 = float(np.log2(np.e) * HEAD_DIM**-0.5)
AW = 640
W_COLS = 1024
PASS1, PASS2 = 3 * 512, 5 * 512
KEYS = 4096
F32, BF16 = jnp.float32, jnp.bfloat16


def rotary_tables():
    inverse = (np.float32(ROTARY_BASE) ** (-np.arange(32, dtype=np.float32) / np.float32(32))).astype(np.float32)
    ang = np.arange(256, dtype=np.float32)[:, None] * inverse
    sign = np.tile(np.array([-1.0, 1.0], np.float32), 32)
    cos = np.repeat(np.cos(ang), 2, axis=1).astype(np.float32)
    sin = np.repeat(np.sin(ang), 2, axis=1).astype(np.float32) * sign
    return cos, sin


class Copy:
    def __init__(self, pool, src, dst, land, dev):
        self.n = pool.take()
        self.pool, self.src, self.dst, self.land, self.dev = pool, src, dst, land, dev

    def start(self):
        self._make(self.src(), self.dst()).start()

    def wait(self):
        here = self.land()
        self._make(here, here).wait_recv()

    def drain(self):
        src = self.src()
        self._make(src, self.dst()).wait_send()

    def _make(self, src, dst):
        return pltpu.make_async_remote_copy(
            src_ref=src, dst_ref=dst, send_sem=self.pool.ssem.at[self.n], recv_sem=self.pool.rsem.at[self.n],
            device_id=self.dev, device_id_type=MESH,
        )


class Phases:
    def __init__(self):
        self.scope = None

    def __call__(self, name):
        if self.scope is not None:
            self.scope.__exit__(None, None, None)
        self.scope = jax.named_scope(name) if name else None
        if name:
            self.scope.__enter__()


class Pool:
    def __init__(self, ssem, rsem, size):
        self.ssem, self.rsem, self.size, self.n, self.all = ssem, rsem, size, 0, []

    def take(self):
        self.n += 1
        assert self.n <= self.size
        return self.n - 1

    def copy(self, src, dst, land, dev):
        c = Copy(self, src, dst, land, dev)
        self.all.append(c)
        return c


N_SEMS = 264


def layer_norm(summed, gain, bias):
    centred = summed - jnp.mean(summed, axis=-1, keepdims=True)
    variance = jnp.mean(centred * centred, axis=-1, keepdims=True)
    return centred * lax.rsqrt(variance + LAYER_EPS) * gain + bias


def norm_rotate(x, gain, cos, sin):
    x = x.astype(F32)
    x = x * lax.rsqrt(jnp.mean(x * x, axis=-1, keepdims=True) + HEAD_EPS) * gain
    even = lax.broadcasted_iota(jnp.int32, x.shape, 1) % 2 == 0
    swapped = jnp.where(even, pltpu.roll(x, HEAD_DIM - 1, 1), pltpu.roll(x, 1, 1))
    return (x * cos + swapped * sin).astype(BF16)


def dot(a, b, dims=((1,), (0,))):
    return lax.dot_general(a, b, (dims, ((), ())), preferred_element_type=F32)


def kernel(
    q_ref, k_ref, v_ref, cosr_ref, cosc_ref, sinr_ref, sinc_ref, qg_ref, kg_ref, fg_ref, fb_ref, sg_ref, sb_ref,
    res_hbm, ow_hbm, up_hbm, dn_hbm,
    out_ref,
    kbuf, vtbuf, qbuf, o_acc, m_acc, l_acc, s_even, s_odd, osend, orecv, stsend, strecv, att_s, attbuf, ow, res, xbuf,
    upbuf, dnbuf, hid, psend, precv, pown, ysend, yrecv, fin,
    ssem, rsem, lsem,
):
    sp, y = lax.axis_index("sp"), lax.axis_index("tp")
    z, x, c = sp // 8, (sp // 2) % 4, sp % 2
    pool = Pool(ssem, rsem, N_SEMS)
    phase = Phases()
    phase("p_prep")

    def dev(dz=0, dx=0, dy=0, flip=False):
        zz, xx, yy = (z + dz + NZ) % NZ, (x + dx + NX) % NX, (y + dy + NY) % NY
        cc = 1 - c if flip else c
        return (zz * 8 + xx * 2 + cc, yy)

    def zat(d):
        return (z + d + NZ) % NZ

    def xat(d):
        return (x + d + NX) % NX

    barrier = pltpu.get_barrier_semaphore()
    partners = [dict(dz=1), dict(dz=-1), dict(dx=1), dict(dx=-1), dict(dx=2), dict(dy=1), dict(dy=-1), dict(dy=2), dict(flip=True)]
    for p in partners:
        pl.semaphore_signal(barrier, inc=1, device_id=dev(**p), device_id_type=MESH)

    def block(zs, xs):
        return pl.multiple_of(zs * 256 + xs * 64, 64)

    mine = pl.multiple_of(c * W_COLS, W_COLS)
    other = pl.multiple_of((1 - c) * W_COLS, W_COLS)
    my_rows = pl.ds(pl.multiple_of(block(z, x) + c * 32, 32), 32)
    partner_rows = pl.ds(pl.multiple_of(block(z, x) + (1 - c) * 32, 32), 32)
    local = [
        pltpu.make_async_copy(up_hbm.at[:, pl.ds(mine, W_COLS)], upbuf.at[my_rows, :], lsem.at[0]),
        pltpu.make_async_copy(dn_hbm.at[:, pl.ds(mine, W_COLS)], dnbuf.at[my_rows, :], lsem.at[1]),
        pltpu.make_async_copy(ow_hbm, ow, lsem.at[2]),
        pltpu.make_async_copy(res_hbm, res, lsem.at[3]),
    ]
    for l in local:
        l.start()

    def angles(rows, cols):
        cols = cols[...]
        parts = [jnp.broadcast_to(rows[pl.ds(sp * 4 + i, 1), :], (GRID_W, HEAD_DIM)) + cols for i in range(4)]
        return jnp.concatenate(parts, axis=0)

    cos, sin = angles(cosr_ref, cosc_ref), angles(sinr_ref, sinc_ref)
    kbuf[0:256, :] = norm_rotate(k_ref[...], kg_ref[...], cos, sin)
    vtbuf[:, 0:256] = jnp.transpose(v_ref[...].astype(F32)).astype(BF16)
    qbuf[0:256, :] = norm_rotate(q_ref[:, 0:128], qg_ref[...], cos, sin)
    qbuf[256:512, :] = norm_rotate(q_ref[:, 128:256], qg_ref[...], cos, sin)

    def same(ref, rows, cols, land_rows, device):
        view = lambda: ref.at[pl.ds(*rows), pl.ds(*cols)]
        return pool.copy(view, view, lambda: ref.at[pl.ds(*land_rows), pl.ds(*cols)], device)

    flip = dev(flip=True)
    KP, KM, KD = {}, {}, {}

    def place(at_key, h):
        return kbuf.at[pl.ds(at_key, 256), :] if h == 0 else vtbuf.at[:, pl.ds(at_key, 256)]

    def ring(src, dst, h, device):
        return pool.copy(lambda: place(src * 512, h), lambda: place(dst * 512, h), lambda: place(dst * 512, h), device)

    for s in range(1, 5):
        for h in range(2):
            if s < 4 or h == 0:
                KP[s, h] = ring(0 if s == 1 else 2 * s - 3, 2 * s - 1, h, dev(dz=1))
            if s < 4 or h == 1:
                KM[s, h] = ring(0 if s == 1 else 2 * s - 2, 2 * s if s < 4 else 7, h, dev(dz=-1))
    class Both(list):
        def start(self):
            for t in self:
                t.start()

        def wait(self):
            for t in self:
                t.wait()

    def to_other(j, h):
        there = lambda: place(j * 512 + 256, h)
        return pool.copy(lambda: place(j * 512, h), there, there, flip)

    for j in range(8):
        KD[j] = Both(to_other(j, h) for h in range(2))
    QS, OS, ST, AT = {}, {}, {}, {}
    for d in range(1, 4):
        QS[d] = pool.copy(
            lambda: qbuf.at[pl.ds(0, 512), :], lambda d=d: qbuf.at[pl.ds(d * 512, 512), :],
            lambda d=d: qbuf.at[pl.ds(d * 512, 512), :], dev(dx=d))
        for h in range(2):
            OS[d, h] = pool.copy(
                lambda d=d, h=h: osend.at[d, h], lambda d=d, h=h: orecv.at[d, h], lambda d=d, h=h: orecv.at[d, h], dev(dx=-d))
        ST[d] = pool.copy(lambda d=d: stsend.at[d], lambda d=d: strecv.at[d], lambda d=d: strecv.at[d], dev(dx=-d))
        AT[d] = pool.copy(
            lambda d=d: att_s.at[pl.ds(pl.multiple_of((y + d) % NY * 64, 64), 64), :],
            lambda d=d: attbuf.at[d], lambda d=d: attbuf.at[d], dev(dy=d))
    def rows_of(ref, lo, n):
        return lambda: ref.at[pl.ds(lo, n), :]

    YP = [pool.copy(rows_of(xbuf, h, 32), rows_of(xbuf, 128 + h, 32), rows_of(xbuf, 128 + h, 32), dev(dy=1)) for h in (0, 32)]
    YM = [pool.copy(rows_of(xbuf, h, 32), rows_of(xbuf, 384 + h, 32), rows_of(xbuf, 384 + h, 32), dev(dy=-1)) for h in (32, 0)]
    YP2 = pool.copy(rows_of(xbuf, 128, 32), rows_of(xbuf, 256, 32), rows_of(xbuf, 256, 32), dev(dy=1))
    YM2 = pool.copy(rows_of(xbuf, 416, 32), rows_of(xbuf, 288, 32), rows_of(xbuf, 288, 32), dev(dy=-1))
    XD = [pool.copy(rows_of(xbuf, j * 128, 64), rows_of(xbuf, j * 128 + 64, 64), rows_of(xbuf, j * 128 + 64, 64), flip) for j in range(4)]

    def exchange(hbm, buf):
        return pool.copy(
            lambda: hbm.at[:, pl.ds(other, W_COLS)], lambda: buf.at[my_rows, :], lambda: buf.at[partner_rows, :], flip)

    WX = {"u": exchange(up_hbm, upbuf), "d": exchange(dn_hbm, dnbuf)}
    order = [0, -1, 1, -2, 2, -3, 3, 4]

    xr = [0, -1, 1, 2]

    class Gather:
        def __init__(self, buf):
            a, b = (0, AW), (AW, W_COLS - AW)
            up, down, right, left = dev(dz=1), dev(dz=-1), dev(dx=1), dev(dx=-1)
            self.AP, self.AM, self.BP, self.BM = {}, {}, {}, {}
            for s in range(1, 5):
                n, h = (64, 0) if s < 4 else (32, 32)
                self.AP[s] = same(buf, (block(zat(1 - s), x), n), a, (block(zat(-s), x), n), up)
                self.AM[s] = same(buf, (block(zat(s - 1), x) + h, n), a, (block(zat(s), x) + h, n), down)
                for i, r in enumerate(xr):
                    if s < 4 or i < 2:
                        self.BP[s, i] = same(buf, (block(zat(1 - s), xat(r)), 64), b, (block(zat(-s), xat(r)), 64), up)
                    if s < 4 or i >= 2:
                        self.BM[s, i] = same(buf, (block(zat(s - 1), xat(r)), 64), b, (block(zat(s), xat(r)), 64), down)
            self.ax = {d: self.spread(buf, zat(d), a, right, left) for d in order}
            self.bx = self.spread(buf, z, b, right, left)

        def spread(self, buf, zs, cols, right, left):
            return (
                same(buf, (block(zs, x), 64), cols, (block(zs, xat(-1)), 64), right),
                same(buf, (block(zs, x), 64), cols, (block(zs, xat(1)), 64), left),
                same(buf, (block(zs, xat(-1)), 32), cols, (block(zs, xat(-2)), 32), right),
                same(buf, (block(zs, xat(1)) + 32, 32), cols, (block(zs, xat(2)) + 32, 32), left),
            )

        def pass_on(self, four):
            four[0].wait()
            four[2].start()
            four[1].wait()
            four[3].start()

        def a_step(self, s):
            self.AP[s].wait()
            if s < 4:
                self.AP[s + 1].start()
            self.AM[s].wait()
            if s < 4:
                self.AM[s + 1].start()
            for d in (-s, s) if s < 4 else (4,):
                self.ax[d][0].start()
                self.ax[d][1].start()

        def b_step(self, s, i):
            for chain in (self.BP, self.BM):
                if (s, i) in chain:
                    chain[s, i].wait()
                    if (s + 1, i) in chain:
                        chain[s + 1, i].start()

        def x_step(self, s):
            for d in (-s, s) if s < 4 else (4,):
                self.pass_on(self.ax[d])

        def have(self, d):
            self.ax[d][2].wait()
            self.ax[d][3].wait()

        def early(self):
            for t in (self.bx[0], self.bx[1], self.ax[0][0], self.ax[0][1]):
                t.start()

        def early_on(self):
            self.pass_on(self.bx)

        def late(self):
            for t in (self.AP[1], self.AM[1], self.BP[1, 0], self.BM[1, 0]):
                t.start()
            self.bx[2].wait()
            self.bx[3].wait()
            for i in (1, 2, 3):
                self.BP[1, i].start()
                self.BM[1, i].start()

        def own_on(self):
            self.pass_on(self.ax[0])

        def groups(self):
            out = [[self.early], [self.early_on, self.late, self.own_on]]
            for s in range(1, 5):
                b = [functools.partial(self.b_step, s, i) for i in range(4)]
                out.append([functools.partial(self.a_step, s), b[0], b[1], functools.partial(self.x_step, s), b[2], b[3]])
            return out

    U, D = Gather(upbuf), Gather(dnbuf)
    DD = [pool.copy(lambda j=j: psend.at[j], lambda j=j: precv.at[j], lambda j=j: precv.at[j], flip) for j in range(8)]
    RS = [
        [pool.copy(lambda j=j, k=k: ysend.at[j, k], lambda j=j, k=k: yrecv.at[j, k], lambda j=j, k=k: yrecv.at[j, k], dev(dy=-k)) for k in (1, 2, 3)]
        for j in range(8)
    ]

    ug, dg = U.groups(), D.groups()
    u, d = sum(ug, []), sum(dg, [])
    names = {id(e): t + str(i) + "_" + str(k) for t, gs in (("u", ug), ("d", dg)) for i, g in enumerate(gs) for k, e in enumerate(g)}

    def run(e):
        with jax.named_scope(names.get(id(e), "step")):
            e()

    def first(g):
        return g[:3]

    def second(g):
        return g[4:]

    def across(g):
        return g[3:4]

    def step(g):
        return first(g) + second(g)

    queue = ug[0] + dg[0] + ug[1] + dg[1][:1] + dg[1][2:] + step(ug[2])
    queue += across(ug[2]) + dg[1][1:2] + step(ug[3]) + across(ug[3]) + step(ug[4]) + step(dg[2])
    queue += across(ug[4]) + step(ug[5]) + across(dg[2]) + across(ug[5]) + step(dg[3])
    queue += across(dg[3]) + step(dg[4]) + across(dg[4]) + step(dg[5]) + across(dg[5])
    d = [e for e in queue if e in d]
    at = [0]

    def w(n):
        for e in queue[at[0] : at[0] + n]:
            run(e)
        at[0] += n

    phase("p_barrier")
    pl.semaphore_wait(barrier, len(partners))
    for h in range(2):
        KP[1, h].start()
        KM[1, h].start()
    KD[0].start()
    for i in (1, 3, 2):
        QS[i].start()
    WX["u"].start()
    WX["d"].start()
    phase("p_wx")
    local[0].wait()
    WX["u"].wait()
    w(1)
    local[1].wait()
    WX["d"].wait()
    w(1)
    phase("p_kv1")
    def kv_step(s):
        for h in range(2):
            for chain in (KP, KM):
                if (s, h) in chain:
                    chain[s, h].wait()
                    if (s + 1, h) in chain:
                        chain[s + 1, h].start()
        if s < 4:
            KD[2 * s - 1].start()
            KD[2 * s].start()
        else:
            KD[7].start()

    kv_step(1)
    for i in range(3):
        KD[i].wait()
    phase("p_qwait")

    def tile_scores(t, at_key, dst, lo, best):
        q = qbuf[pl.ds(pl.multiple_of(t * 256, 256), 256), :]
        part = dot(kbuf[pl.ds(at_key, 512), :], q, ((1,), (1,)))
        dst[pl.ds(at_key - lo, 512), :] = part
        top = jnp.max(part.reshape(64, 8, 256), axis=0)
        return top if best is None else jnp.maximum(best, top)

    def stage(t_next, t, src, dst, m, lo, hi):
        best, total, out = None, None, None
        for at_key in range(lo, hi, 512):
            best = tile_scores(t_next, at_key, dst, lo, best)
            p = jnp.exp2((src[pl.ds(at_key - lo, 512), :] - m) * SCALE2)
            part = jnp.sum(p.reshape(64, 8, 256), axis=0)
            o = dot(vtbuf[:, pl.ds(at_key, 512)], p.astype(BF16))
            total, out = (part, o) if total is None else (total + part, out + o)
        l = jnp.sum(total, axis=0, keepdims=True)
        m_next = jnp.max(best, axis=0, keepdims=True)
        if lo > 0:
            m_old = m_acc[t, 0:1, :]
            alpha = jnp.exp2((m_old - m) * SCALE2)
            out = o_acc[t] * alpha + out
            l = l_acc[t, 0:1, :] * alpha + l
            m_next = jnp.maximum(m_next, m_acc[t_next, 0:1, :])
        if hi == KEYS:
            upper = lax.broadcasted_iota(jnp.int32, (8, 256), 0) < 4
            stsend[t // 2, t % 2] = jnp.where(upper, jnp.broadcast_to(m, (8, 256)), jnp.broadcast_to(l, (8, 256)))
            osend[t // 2, t % 2] = out.astype(BF16)
        o_acc[t] = out
        m_acc[t] = jnp.broadcast_to(m, (8, 256))
        l_acc[t] = jnp.broadcast_to(l, (8, 256))
        return m_next

    def all_tiles(lo, hi, table):
        def slot_of(i):
            return (2 + i * (i + 1) // 2) % 4 if hi == KEYS else i % 4

        best, t = None, 2 * slot_of(0)
        for at_key in range(lo, hi, 512):
            best = tile_scores(t, at_key, s_even, lo, best)
        m = jnp.max(best, axis=0, keepdims=True)
        if lo > 0:
            m = jnp.maximum(m, m_acc[t, 0:1, :])

        def two(i, m):
            t = 2 * slot_of(i)
            m = stage(t + 1, t, s_even, s_odd, m, lo, hi)
            events_at(i, {k // 2: f for k, f in table.items() if k % 2 == 0})
            m = stage(2 * slot_of(i + 1), t + 1, s_odd, s_even, m, lo, hi)
            events_at(i, {k // 2: f for k, f in table.items() if k % 2 == 1})
            return m

        lax.fori_loop(0, 4, two, m)

    def events_at(i, table):
        for step, fns in table.items():
            @pl.when(i == step)
            def _(fns=fns):
                for f in fns:
                    run(f)

    def grab(n):
        got = queue[at[0] : at[0] + n]
        at[0] += n
        return got

    def queries_from(*who):
        return [lambda: [QS[i].wait() for i in who]]

    ev1 = {
        0: queries_from(1, 3) + grab(1), 1: [lambda: kv_step(2)], 2: queries_from(2) + grab(1), 4: grab(1), 5: grab(1), 6: grab(1),
    }
    ev2 = {0: [lambda: kv_step(3)], 7: [lambda: kv_step(4)]}
    phase("p_pass1")
    all_tiles(0, PASS1, ev1)
    phase("p_pass1b")
    for i in (3, 4):
        KD[i].wait()
    all_tiles(PASS1, PASS2, ev2)
    phase("p_kdwait")
    w(5)
    for i in (5, 6, 7):
        KD[i].wait()

    def send_o(d, h):
        def go():
            OS[d, h].start()
            if h == 1:
                ST[d].start()

        return [go]

    ev3 = {2 * i + h: send_o(d, h) for i, d in enumerate((2, 3, 1)) for h in range(2)}
    for k, n in ((1, 1), (3, 1), (5, 3)):
        ev3[k] = ev3[k] + grab(n)
    phase("p_pass2")
    all_tiles(PASS2, KEYS, ev3)

    phase("p_owait")
    w(2)
    for i in (1, 2, 3):
        ST[i].wait()
    for i in (1, 2, 3):
        OS[i, 0].wait()
        OS[i, 1].wait()
    phase("p_combine")
    for h in range(2):
        ms, ls = [m_acc[h, 0:1, :]], [l_acc[h, 0:1, :]]
        for i in (1, 2, 3):
            ms.append(strecv[i, h, 0:1, :])
            ls.append(strecv[i, h, 4:5, :])
        top = jnp.maximum(jnp.maximum(ms[0], ms[1]), jnp.maximum(ms[2], ms[3]))
        es = [jnp.exp2((m - top) * SCALE2) for m in ms]
        num = o_acc[h] * es[0]
        den = ls[0] * es[0]
        for i in (1, 2, 3):
            num += orecv[i, h].astype(F32) * es[i]
            den += ls[i] * es[i]
        att_s[:, h * 128 : h * 128 + 128] = jnp.transpose(num / den).astype(BF16)
    phase("p_att")
    for i in (1, 3, 2):
        AT[i].start()
    local[2].wait()
    local[3].wait()
    w(11)
    phase("q_atwait")
    for i in (1, 2, 3):
        AT[i].wait()
    phase("p_mixed")
    mixed = RESIDUAL_SCALE * res[...].astype(F32)
    for i in range(4):
        a = att_s[pl.ds(pl.multiple_of(y * 64, 64), 64), :] if i == 0 else attbuf[i]
        mixed += dot(a, ow[pl.ds(pl.multiple_of((y - i + NY) % NY * 256, 256), 256), :])
    xbuf[0:64, :] = layer_norm(mixed, fg_ref[...], fb_ref[...]).astype(BF16)
    phase("p_yag")
    for t in (YP[0], YM[0], YP[1], YM[1], XD[0]):
        t.start()
    w(7)
    phase("q_yp1")
    YP[0].wait()
    YP2.start()
    YM[0].wait()
    YM2.start()
    YP[1].wait()
    XD[1].start()
    YM[1].wait()
    XD[3].start()
    w(6)
    assert not any(e in u for e in queue[at[0] :])
    YP2.wait()
    YM2.wait()
    XD[2].start()
    phase("q_uhave")
    for i in order:
        U.have(i)

    def up_rows(lo, n):
        def tile(i, _):
            cols = pl.ds(pl.multiple_of(i * 256, 256), 256)
            h = jnp.maximum(dot(xbuf[pl.ds(lo, n), :], upbuf[:, cols]), 0.0)
            hid[pl.ds(lo, n), cols] = (h * h).astype(BF16)
            return 0

        lax.fori_loop(0, 4, tile, 0)

    phase("q_up0")
    XD[0].wait()
    XD[1].wait()
    up_rows(0, 256)
    w(4)
    phase("q_xd")
    XD[3].wait()
    XD[2].wait()
    phase("q_up2")
    up_rows(256, 256)
    w(2)

    def combine(j, zs):
        phase("q_ddwait")
        DD[j].wait()
        phase("q_comb")
        cols = pl.ds(pl.multiple_of(zs * 256, 256), 256)
        both = pown[j % 2] + precv[j].astype(F32)
        fin[:, cols] = both[0:64]
        for k in (1, 2, 3):
            ysend[j, k] = both[k * 64 : k * 64 + 64].astype(BF16)
        for k in (1, 3, 2):
            RS[j][k - 1].start()

    phase("p_down")
    need = {dz: max(i for i, e in enumerate(d) if any(e in g for g in dg[: abs(dz) + 2])) + 1 for dz in order}
    ahead = {0: len(d) - 7, 1: len(d) - 3, 2: len(d) - 1, 3: len(d) - 1}
    done_d = [len([f for f in d if f not in queue[at[0] :]])]
    for j, dz in enumerate(order):
        while done_d[0] < max(need[dz], ahead.get(j, len(d))):
            run(d[done_d[0]])
            done_d[0] += 1
        phase("q_have")
        D.have(dz)
        phase("q_dot")
        zs = zat(dz)
        part = dot(hid[...], dnbuf[pl.ds(pl.multiple_of(zs * 256, 256), 256), :], ((1,), (1,)))
        for i in range(4):
            pown[j % 2, i * 64 : i * 64 + 64, :] = part[i * 128 : i * 128 + 64]
            psend[j, i * 64 : i * 64 + 64, :] = part[i * 128 + 64 : i * 128 + 128].astype(BF16)
        DD[j].start()
        if j > 0:
            combine(j - 1, zat(order[j - 1]))
    combine(7, zat(4))

    phase("p_last")
    for j, dz in enumerate(order):
        cols = pl.ds(pl.multiple_of(zat(dz) * 256, 256), 256)
        phase("q_rswait")
        for k in (1, 2, 3):
            RS[j][k - 1].wait()
        phase("q_fin")
        fin[:, cols] = fin[:, cols] + (yrecv[j, 1].astype(F32) + yrecv[j, 2].astype(F32) + yrecv[j, 3].astype(F32))
    summed = RESIDUAL_SCALE * xbuf[0:64, :].astype(F32) + fin[...]
    out_ref[...] = layer_norm(summed, sg_ref[...], sb_ref[...]).astype(BF16)
    phase("p_drain")
    for t in pool.all:
        t.drain()
    phase(None)


def per_device(
    queries, keys, values, residual, query_gain, key_gain, out_weight, first_gain, first_bias, up_weight, down_weight,
    second_gain, second_bias,
):
    cos, sin = rotary_tables()
    zero = np.zeros((256, 64), np.float32)

    def table(t):
        return jnp.asarray(np.concatenate([t, zero], 1)), jnp.asarray(np.concatenate([zero, t], 1)[:GRID_W])

    vmem, hbm = pl.BlockSpec(memory_space=pltpu.VMEM), pl.BlockSpec(memory_space=pl.ANY)
    scratch = [
        pltpu.VMEM((KEYS, 128), BF16),
        pltpu.VMEM((128, KEYS), BF16),
        pltpu.VMEM((2048, 128), BF16),
        pltpu.VMEM((8, 128, 256), F32),
        pltpu.VMEM((8, 8, 256), F32),
        pltpu.VMEM((8, 8, 256), F32),
        pltpu.VMEM((1536, 256), F32),
        pltpu.VMEM((1536, 256), F32),
        pltpu.VMEM((4, 2, 128, 256), BF16),
        pltpu.VMEM((4, 2, 128, 256), BF16),
        pltpu.VMEM((4, 2, 8, 256), F32),
        pltpu.VMEM((4, 2, 8, 256), F32),
        pltpu.VMEM((256, 256), BF16),
        pltpu.VMEM((4, 64, 256), BF16),
        pltpu.VMEM((1024, 2048), BF16),
        pltpu.VMEM((64, 2048), BF16),
        pltpu.VMEM((512, 2048), BF16),
        pltpu.VMEM((2048, W_COLS), BF16),
        pltpu.VMEM((2048, W_COLS), BF16),
        pltpu.VMEM((512, W_COLS), BF16),
        pltpu.VMEM((8, 256, 256), BF16),
        pltpu.VMEM((8, 256, 256), BF16),
        pltpu.VMEM((2, 256, 256), F32),
        pltpu.VMEM((8, 4, 64, 256), BF16),
        pltpu.VMEM((8, 4, 64, 256), BF16),
        pltpu.VMEM((64, 2048), F32),
        pltpu.SemaphoreType.DMA((N_SEMS,)),
        pltpu.SemaphoreType.DMA((N_SEMS,)),
        pltpu.SemaphoreType.DMA((4,)),
    ]
    return pl.pallas_call(
        kernel,
        out_shape=jax.ShapeDtypeStruct((64, 2048), BF16),
        in_specs=[vmem] * 13 + [hbm] * 4,
        out_specs=vmem,
        scratch_shapes=scratch,
        compiler_params=pltpu.CompilerParams(collective_id=0, has_side_effects=True, vmem_limit_bytes=62 * 1024 * 1024),
        name="layer",
    )(
        queries, keys, values, *table(cos), *table(sin), query_gain[None], key_gain[None], first_gain[None], first_bias[None],
        second_gain[None], second_bias[None], residual, out_weight, up_weight, down_weight,
    )


def solution(mesh):
    in_specs = (
        P("sp", "tp"), P("sp", "tp"), P("sp", "tp"), P(("sp", "tp"), None), P(), P(), P(), P(), P(),
        P("sp", "tp"), P("sp", "tp"), P(), P(),
    )
    return jax.shard_map(per_device, mesh=mesh, in_specs=in_specs, out_specs=P(("sp", "tp"), None), check_vma=False)
```

```python
import functools

import jax
import jax.numpy as jnp
import numpy as np
from jax import lax
from jax.experimental import pallas as pl
from jax.experimental.pallas import tpu as pltpu
from jax.sharding import PartitionSpec as P

MESH = pl.DeviceIdType.MESH
HEAD_DIM = 128
GRID_W = 64
RESIDUAL_SCALE = 2.0**0.25
LAYER_EPS = 1e-05
HEAD_EPS = 1e-06
ROTARY_BASE = 10000.0
NZ, NX, NC, NY = 8, 4, 2, 4
SCALE2 = float(np.log2(np.e) * HEAD_DIM**-0.5)
AW = 640
W_COLS = 1024
PASS1, PASS2 = 3 * 512, 5 * 512
KEYS = 4096
F32, BF16 = jnp.float32, jnp.bfloat16


def rotary_tables():
    inverse = (np.float32(ROTARY_BASE) ** (-np.arange(32, dtype=np.float32) / np.float32(32))).astype(np.float32)
    ang = np.arange(256, dtype=np.float32)[:, None] * inverse
    sign = np.tile(np.array([-1.0, 1.0], np.float32), 32)
    cos = np.repeat(np.cos(ang), 2, axis=1).astype(np.float32)
    sin = np.repeat(np.sin(ang), 2, axis=1).astype(np.float32) * sign
    return cos, sin


class Copy:
    def __init__(self, pool, src, dst, land, dev):
        self.n = pool.take()
        self.pool, self.src, self.dst, self.land, self.dev = pool, src, dst, land, dev

    def start(self):
        self._make(self.src(), self.dst()).start()

    def wait(self):
        here = self.land()
        self._make(here, here).wait_recv()

    def drain(self):
        src = self.src()
        self._make(src, self.dst()).wait_send()

    def _make(self, src, dst):
        return pltpu.make_async_remote_copy(
            src_ref=src, dst_ref=dst, send_sem=self.pool.ssem.at[self.n], recv_sem=self.pool.rsem.at[self.n],
            device_id=self.dev, device_id_type=MESH,
        )


class Phases:
    def __init__(self):
        self.scope = None

    def __call__(self, name):
        if self.scope is not None:
            self.scope.__exit__(None, None, None)
        self.scope = jax.named_scope(name) if name else None
        if name:
            self.scope.__enter__()


class Pool:
    def __init__(self, ssem, rsem, size):
        self.ssem, self.rsem, self.size, self.n, self.all = ssem, rsem, size, 0, []

    def take(self):
        self.n += 1
        assert self.n <= self.size
        return self.n - 1

    def copy(self, src, dst, land, dev):
        c = Copy(self, src, dst, land, dev)
        self.all.append(c)
        return c


N_SEMS = 264


def layer_norm(summed, gain, bias):
    centred = summed - jnp.mean(summed, axis=-1, keepdims=True)
    variance = jnp.mean(centred * centred, axis=-1, keepdims=True)
    return centred * lax.rsqrt(variance + LAYER_EPS) * gain + bias


def norm_rotate(x, gain, cos, sin):
    x = x.astype(F32)
    x = x * lax.rsqrt(jnp.mean(x * x, axis=-1, keepdims=True) + HEAD_EPS) * gain
    even = lax.broadcasted_iota(jnp.int32, x.shape, 1) % 2 == 0
    swapped = jnp.where(even, pltpu.roll(x, HEAD_DIM - 1, 1), pltpu.roll(x, 1, 1))
    return (x * cos + swapped * sin).astype(BF16)


def dot(a, b, dims=((1,), (0,))):
    return lax.dot_general(a, b, (dims, ((), ())), preferred_element_type=F32)


def kernel(
    q_ref, k_ref, v_ref, cosr_ref, cosc_ref, sinr_ref, sinc_ref, qg_ref, kg_ref, fg_ref, fb_ref, sg_ref, sb_ref,
    res_hbm, ow_hbm, up_hbm, dn_hbm,
    out_ref,
    kbuf, vtbuf, qbuf, o_acc, m_acc, l_acc, s_even, s_odd, osend, orecv, stsend, strecv, att_s, attbuf, ow, res, xbuf,
    upbuf, dnbuf, hid, psend, precv, pown, ysend, yrecv, fin,
    ssem, rsem, lsem,
):
    sp, y = lax.axis_index("sp"), lax.axis_index("tp")
    z, x, c = sp // 8, (sp // 2) % 4, sp % 2
    pool = Pool(ssem, rsem, N_SEMS)
    phase = Phases()
    phase("p_prep")

    def dev(dz=0, dx=0, dy=0, flip=False):
        zz, xx, yy = (z + dz + NZ) % NZ, (x + dx + NX) % NX, (y + dy + NY) % NY
        cc = 1 - c if flip else c
        return (zz * 8 + xx * 2 + cc, yy)

    def zat(d):
        return (z + d + NZ) % NZ

    def xat(d):
        return (x + d + NX) % NX

    barrier = pltpu.get_barrier_semaphore()
    partners = [dict(dz=1), dict(dz=-1), dict(dx=1), dict(dx=-1), dict(dx=2), dict(dy=1), dict(dy=-1), dict(dy=2), dict(flip=True)]
    for p in partners:
        pl.semaphore_signal(barrier, inc=1, device_id=dev(**p), device_id_type=MESH)

    def block(zs, xs):
        return pl.multiple_of(zs * 256 + xs * 64, 64)

    mine = pl.multiple_of(c * W_COLS, W_COLS)
    other = pl.multiple_of((1 - c) * W_COLS, W_COLS)
    my_rows = pl.ds(pl.multiple_of(block(z, x) + c * 32, 32), 32)
    partner_rows = pl.ds(pl.multiple_of(block(z, x) + (1 - c) * 32, 32), 32)
    local = [
        pltpu.make_async_copy(up_hbm.at[:, pl.ds(mine, W_COLS)], upbuf.at[my_rows, :], lsem.at[0]),
        pltpu.make_async_copy(dn_hbm.at[:, pl.ds(mine, W_COLS)], dnbuf.at[my_rows, :], lsem.at[1]),
        pltpu.make_async_copy(ow_hbm, ow, lsem.at[2]),
        pltpu.make_async_copy(res_hbm, res, lsem.at[3]),
    ]
    for l in local:
        l.start()

    def angles(rows, cols):
        cols = cols[...]
        parts = [jnp.broadcast_to(rows[pl.ds(sp * 4 + i, 1), :], (GRID_W, HEAD_DIM)) + cols for i in range(4)]
        return jnp.concatenate(parts, axis=0)

    cos, sin = angles(cosr_ref, cosc_ref), angles(sinr_ref, sinc_ref)
    kbuf[0:256, :] = norm_rotate(k_ref[...], kg_ref[...], cos, sin)
    vtbuf[:, 0:256] = jnp.transpose(v_ref[...].astype(F32)).astype(BF16)
    qbuf[0:256, :] = norm_rotate(q_ref[:, 0:128], qg_ref[...], cos, sin)
    qbuf[256:512, :] = norm_rotate(q_ref[:, 128:256], qg_ref[...], cos, sin)

    def same(ref, rows, cols, land_rows, device):
        view = lambda: ref.at[pl.ds(*rows), pl.ds(*cols)]
        return pool.copy(view, view, lambda: ref.at[pl.ds(*land_rows), pl.ds(*cols)], device)

    flip = dev(flip=True)
    KP, KM, KD = {}, {}, {}

    def place(at_key, h):
        return kbuf.at[pl.ds(at_key, 256), :] if h == 0 else vtbuf.at[:, pl.ds(at_key, 256)]

    def ring(src, dst, h, device):
        return pool.copy(lambda: place(src * 512, h), lambda: place(dst * 512, h), lambda: place(dst * 512, h), device)

    for s in range(1, 5):
        for h in range(2):
            if s < 4 or h == 0:
                KP[s, h] = ring(0 if s == 1 else 2 * s - 3, 2 * s - 1, h, dev(dz=1))
            if s < 4 or h == 1:
                KM[s, h] = ring(0 if s == 1 else 2 * s - 2, 2 * s if s < 4 else 7, h, dev(dz=-1))
    class Both(list):
        def start(self):
            for t in self:
                t.start()

        def wait(self):
            for t in self:
                t.wait()

    def to_other(j, h):
        there = lambda: place(j * 512 + 256, h)
        return pool.copy(lambda: place(j * 512, h), there, there, flip)

    for j in range(8):
        KD[j] = Both(to_other(j, h) for h in range(2))
    QS, OS, ST, AT = {}, {}, {}, {}
    for d in range(1, 4):
        QS[d] = pool.copy(
            lambda: qbuf.at[pl.ds(0, 512), :], lambda d=d: qbuf.at[pl.ds(d * 512, 512), :],
            lambda d=d: qbuf.at[pl.ds(d * 512, 512), :], dev(dx=d))
        for h in range(2):
            OS[d, h] = pool.copy(
                lambda d=d, h=h: osend.at[d, h], lambda d=d, h=h: orecv.at[d, h], lambda d=d, h=h: orecv.at[d, h], dev(dx=-d))
        ST[d] = pool.copy(lambda d=d: stsend.at[d], lambda d=d: strecv.at[d], lambda d=d: strecv.at[d], dev(dx=-d))
        AT[d] = pool.copy(
            lambda d=d: att_s.at[pl.ds(pl.multiple_of((y + d) % NY * 64, 64), 64), :],
            lambda d=d: attbuf.at[d], lambda d=d: attbuf.at[d], dev(dy=d))
    def rows_of(ref, lo, n):
        return lambda: ref.at[pl.ds(lo, n), :]

    YP = [pool.copy(rows_of(xbuf, h, 32), rows_of(xbuf, 128 + h, 32), rows_of(xbuf, 128 + h, 32), dev(dy=1)) for h in (0, 32)]
    YM = [pool.copy(rows_of(xbuf, h, 32), rows_of(xbuf, 384 + h, 32), rows_of(xbuf, 384 + h, 32), dev(dy=-1)) for h in (32, 0)]
    YP2 = pool.copy(rows_of(xbuf, 128, 32), rows_of(xbuf, 256, 32), rows_of(xbuf, 256, 32), dev(dy=1))
    YM2 = pool.copy(rows_of(xbuf, 416, 32), rows_of(xbuf, 288, 32), rows_of(xbuf, 288, 32), dev(dy=-1))
    XD = [pool.copy(rows_of(xbuf, j * 128, 64), rows_of(xbuf, j * 128 + 64, 64), rows_of(xbuf, j * 128 + 64, 64), flip) for j in range(4)]

    def exchange(hbm, buf):
        return pool.copy(
            lambda: hbm.at[:, pl.ds(other, W_COLS)], lambda: buf.at[my_rows, :], lambda: buf.at[partner_rows, :], flip)

    WX = {"u": exchange(up_hbm, upbuf), "d": exchange(dn_hbm, dnbuf)}
    order = [0, -1, 1, -2, 2, -3, 3, 4]

    xr = [0, -1, 1, 2]

    class Gather:
        def __init__(self, buf):
            a, b = (0, AW), (AW, W_COLS - AW)
            up, down, right, left = dev(dz=1), dev(dz=-1), dev(dx=1), dev(dx=-1)
            self.AP, self.AM, self.BP, self.BM = {}, {}, {}, {}
            for s in range(1, 5):
                n, h = (64, 0) if s < 4 else (32, 32)
                self.AP[s] = same(buf, (block(zat(1 - s), x), n), a, (block(zat(-s), x), n), up)
                self.AM[s] = same(buf, (block(zat(s - 1), x) + h, n), a, (block(zat(s), x) + h, n), down)
                for i, r in enumerate(xr):
                    if s < 4 or i < 2:
                        self.BP[s, i] = same(buf, (block(zat(1 - s), xat(r)), 64), b, (block(zat(-s), xat(r)), 64), up)
                    if s < 4 or i >= 2:
                        self.BM[s, i] = same(buf, (block(zat(s - 1), xat(r)), 64), b, (block(zat(s), xat(r)), 64), down)
            self.ax = {d: self.spread(buf, zat(d), a, right, left) for d in order}
            self.bx = self.spread(buf, z, b, right, left)

        def spread(self, buf, zs, cols, right, left):
            return (
                same(buf, (block(zs, x), 64), cols, (block(zs, xat(-1)), 64), right),
                same(buf, (block(zs, x), 64), cols, (block(zs, xat(1)), 64), left),
                same(buf, (block(zs, xat(-1)), 32), cols, (block(zs, xat(-2)), 32), right),
                same(buf, (block(zs, xat(1)) + 32, 32), cols, (block(zs, xat(2)) + 32, 32), left),
            )

        def pass_on(self, four):
            four[0].wait()
            four[2].start()
            four[1].wait()
            four[3].start()

        def a_step(self, s):
            self.AP[s].wait()
            if s < 4:
                self.AP[s + 1].start()
            self.AM[s].wait()
            if s < 4:
                self.AM[s + 1].start()
            for d in (-s, s) if s < 4 else (4,):
                self.ax[d][0].start()
                self.ax[d][1].start()

        def b_step(self, s, i):
            for chain in (self.BP, self.BM):
                if (s, i) in chain:
                    chain[s, i].wait()
                    if (s + 1, i) in chain:
                        chain[s + 1, i].start()

        def x_step(self, s):
            for d in (-s, s) if s < 4 else (4,):
                self.pass_on(self.ax[d])

        def have(self, d):
            self.ax[d][2].wait()
            self.ax[d][3].wait()

        def early(self):
            for t in (self.bx[0], self.bx[1], self.ax[0][0], self.ax[0][1]):
                t.start()

        def early_on(self):
            self.pass_on(self.bx)

        def late(self):
            for t in (self.AP[1], self.AM[1], self.BP[1, 0], self.BM[1, 0]):
                t.start()
            self.bx[2].wait()
            self.bx[3].wait()
            for i in (1, 2, 3):
                self.BP[1, i].start()
                self.BM[1, i].start()

        def own_on(self):
            self.pass_on(self.ax[0])

        def groups(self):
            out = [[self.early], [self.early_on, self.late, self.own_on]]
            for s in range(1, 5):
                b = [functools.partial(self.b_step, s, i) for i in range(4)]
                out.append([functools.partial(self.a_step, s), b[0], b[1], functools.partial(self.x_step, s), b[2], b[3]])
            return out

    U, D = Gather(upbuf), Gather(dnbuf)
    DD = [pool.copy(lambda j=j: psend.at[j], lambda j=j: precv.at[j], lambda j=j: precv.at[j], flip) for j in range(8)]
    RS = [
        [pool.copy(lambda j=j, k=k: ysend.at[j, k], lambda j=j, k=k: yrecv.at[j, k], lambda j=j, k=k: yrecv.at[j, k], dev(dy=-k)) for k in (1, 2, 3)]
        for j in range(8)
    ]

    ug, dg = U.groups(), D.groups()
    u, d = sum(ug, []), sum(dg, [])
    names = {id(e): t + str(i) + "_" + str(k) for t, gs in (("u", ug), ("d", dg)) for i, g in enumerate(gs) for k, e in enumerate(g)}

    def run(e):
        with jax.named_scope(names.get(id(e), "step")):
            e()

    def first(g):
        return g[:3]

    def second(g):
        return g[4:]

    def across(g):
        return g[3:4]

    def step(g):
        return first(g) + second(g)

    queue = ug[0] + dg[0] + ug[1] + dg[1][:1] + dg[1][2:] + step(ug[2])
    queue += across(ug[2]) + dg[1][1:2] + step(ug[3]) + across(ug[3]) + step(ug[4]) + step(dg[2])
    queue += across(ug[4]) + step(ug[5]) + across(dg[2]) + across(ug[5]) + step(dg[3])
    queue += across(dg[3]) + step(dg[4]) + across(dg[4]) + step(dg[5]) + across(dg[5])
    d = [e for e in queue if e in d]
    at = [0]

    def w(n):
        for e in queue[at[0] : at[0] + n]:
            run(e)
        at[0] += n

    phase("p_barrier")
    pl.semaphore_wait(barrier, len(partners))
    for h in range(2):
        KP[1, h].start()
        KM[1, h].start()
    KD[0].start()
    for i in (1, 3, 2):
        QS[i].start()
    WX["u"].start()
    WX["d"].start()
    phase("p_wx")
    local[0].wait()
    WX["u"].wait()
    w(1)
    local[1].wait()
    WX["d"].wait()
    w(1)
    phase("p_kv1")
    def kv_step(s):
        for h in range(2):
            for chain in (KP, KM):
                if (s, h) in chain:
                    chain[s, h].wait()
                    if (s + 1, h) in chain:
                        chain[s + 1, h].start()
        if s < 4:
            KD[2 * s - 1].start()
            KD[2 * s].start()
        else:
            KD[7].start()

    kv_step(1)
    for i in range(3):
        KD[i].wait()
    phase("p_qwait")

    def tile_scores(t, at_key, dst, lo, best):
        q = qbuf[pl.ds(pl.multiple_of(t * 256, 256), 256), :]
        part = dot(kbuf[pl.ds(at_key, 512), :], q, ((1,), (1,)))
        dst[pl.ds(at_key - lo, 512), :] = part
        top = jnp.max(part.reshape(64, 8, 256), axis=0)
        return top if best is None else jnp.maximum(best, top)

    def stage(t_next, t, src, dst, m, lo, hi):
        best, total, out = None, None, None
        for at_key in range(lo, hi, 512):
            best = tile_scores(t_next, at_key, dst, lo, best)
            p = jnp.exp2((src[pl.ds(at_key - lo, 512), :] - m) * SCALE2)
            part = jnp.sum(p.reshape(64, 8, 256), axis=0)
            o = dot(vtbuf[:, pl.ds(at_key, 512)], p.astype(BF16))
            total, out = (part, o) if total is None else (total + part, out + o)
        l = jnp.sum(total, axis=0, keepdims=True)
        m_next = jnp.max(best, axis=0, keepdims=True)
        if lo > 0:
            m_old = m_acc[t, 0:1, :]
            alpha = jnp.exp2((m_old - m) * SCALE2)
            out = o_acc[t] * alpha + out
            l = l_acc[t, 0:1, :] * alpha + l
            m_next = jnp.maximum(m_next, m_acc[t_next, 0:1, :])
        if hi == KEYS:
            upper = lax.broadcasted_iota(jnp.int32, (8, 256), 0) < 4
            stsend[t // 2, t % 2] = jnp.where(upper, jnp.broadcast_to(m, (8, 256)), jnp.broadcast_to(l, (8, 256)))
            osend[t // 2, t % 2] = out.astype(BF16)
        o_acc[t] = out
        m_acc[t] = jnp.broadcast_to(m, (8, 256))
        l_acc[t] = jnp.broadcast_to(l, (8, 256))
        return m_next

    def all_tiles(lo, hi, table):
        def slot_of(i):
            return (2 + i * (i + 1) // 2) % 4 if hi == KEYS else i % 4

        best, t = None, 2 * slot_of(0)
        for at_key in range(lo, hi, 512):
            best = tile_scores(t, at_key, s_even, lo, best)
        m = jnp.max(best, axis=0, keepdims=True)
        if lo > 0:
            m = jnp.maximum(m, m_acc[t, 0:1, :])

        def two(i, m):
            t = 2 * slot_of(i)
            m = stage(t + 1, t, s_even, s_odd, m, lo, hi)
            events_at(i, {k // 2: f for k, f in table.items() if k % 2 == 0})
            m = stage(2 * slot_of(i + 1), t + 1, s_odd, s_even, m, lo, hi)
            events_at(i, {k // 2: f for k, f in table.items() if k % 2 == 1})
            return m

        lax.fori_loop(0, 4, two, m)

    def events_at(i, table):
        for step, fns in table.items():
            @pl.when(i == step)
            def _(fns=fns):
                for f in fns:
                    run(f)

    def grab(n):
        got = queue[at[0] : at[0] + n]
        at[0] += n
        return got

    def queries_from(*who):
        return [lambda: [QS[i].wait() for i in who]]

    ev1 = {
        0: queries_from(1, 3) + grab(1), 1: [lambda: kv_step(2)], 2: queries_from(2) + grab(1), 4: grab(1), 5: grab(1), 6: grab(1),
    }
    ev2 = {0: [lambda: kv_step(3)], 7: [lambda: kv_step(4)]}
    phase("p_pass1")
    all_tiles(0, PASS1, ev1)
    phase("p_pass1b")
    for i in (3, 4):
        KD[i].wait()
    all_tiles(PASS1, PASS2, ev2)
    phase("p_kdwait")
    w(5)
    for i in (5, 6, 7):
        KD[i].wait()

    def send_o(d, h):
        def go():
            OS[d, h].start()
            if h == 1:
                ST[d].start()

        return [go]

    ev3 = {2 * i + h: send_o(d, h) for i, d in enumerate((2, 3, 1)) for h in range(2)}
    for k, n in ((1, 1), (3, 1), (5, 3)):
        ev3[k] = ev3[k] + grab(n)
    phase("p_pass2")
    all_tiles(PASS2, KEYS, ev3)

    phase("p_owait")
    w(2)
    for i in (1, 2, 3):
        ST[i].wait()
    for i in (1, 2, 3):
        OS[i, 0].wait()
        OS[i, 1].wait()
    phase("p_combine")
    for h in range(2):
        ms, ls = [m_acc[h, 0:1, :]], [l_acc[h, 0:1, :]]
        for i in (1, 2, 3):
            ms.append(strecv[i, h, 0:1, :])
            ls.append(strecv[i, h, 4:5, :])
        top = jnp.maximum(jnp.maximum(ms[0], ms[1]), jnp.maximum(ms[2], ms[3]))
        es = [jnp.exp2((m - top) * SCALE2) for m in ms]
        num = o_acc[h] * es[0]
        den = ls[0] * es[0]
        for i in (1, 2, 3):
            num += orecv[i, h].astype(F32) * es[i]
            den += ls[i] * es[i]
        att_s[:, h * 128 : h * 128 + 128] = jnp.transpose(num / den).astype(BF16)
    phase("p_att")
    for i in (1, 3, 2):
        AT[i].start()
    local[2].wait()
    local[3].wait()
    w(11)
    phase("q_atwait")
    for i in (1, 2, 3):
        AT[i].wait()
    phase("p_mixed")
    mixed = RESIDUAL_SCALE * res[...].astype(F32)
    for i in range(4):
        a = att_s[pl.ds(pl.multiple_of(y * 64, 64), 64), :] if i == 0 else attbuf[i]
        mixed += dot(a, ow[pl.ds(pl.multiple_of((y - i + NY) % NY * 256, 256), 256), :])
    xbuf[0:64, :] = layer_norm(mixed, fg_ref[...], fb_ref[...]).astype(BF16)
    phase("p_yag")
    for t in (YP[0], YM[0], YP[1], YM[1], XD[0]):
        t.start()
    w(7)
    phase("q_yp1")
    YP[0].wait()
    YP2.start()
    YM[0].wait()
    YM2.start()
    YP[1].wait()
    XD[1].start()
    YM[1].wait()
    XD[3].start()
    w(6)
    assert not any(e in u for e in queue[at[0] :])
    YP2.wait()
    YM2.wait()
    XD[2].start()
    phase("q_uhave")
    for i in order:
        U.have(i)

    def up_rows(lo, n):
        def tile(i, _):
            cols = pl.ds(pl.multiple_of(i * 256, 256), 256)
            h = jnp.maximum(dot(xbuf[pl.ds(lo, n), :], upbuf[:, cols]), 0.0)
            hid[pl.ds(lo, n), cols] = (h * h).astype(BF16)
            return 0

        lax.fori_loop(0, 4, tile, 0)

    phase("q_up0")
    XD[0].wait()
    XD[1].wait()
    up_rows(0, 256)
    w(4)
    phase("q_xd")
    XD[3].wait()
    XD[2].wait()
    phase("q_up2")
    up_rows(256, 256)
    w(2)

    def combine(j, zs):
        phase("q_ddwait")
        DD[j].wait()
        phase("q_comb")
        cols = pl.ds(pl.multiple_of(zs * 256, 256), 256)
        both = pown[j % 2] + precv[j].astype(F32)
        fin[:, cols] = both[0:64]
        for k in (1, 2, 3):
            ysend[j, k] = both[k * 64 : k * 64 + 64].astype(BF16)
        for k in (1, 3, 2):
            RS[j][k - 1].start()

    phase("p_down")
    need = {dz: max(i for i, e in enumerate(d) if any(e in g for g in dg[: abs(dz) + 2])) + 1 for dz in order}
    ahead = {0: len(d) - 7, 1: len(d) - 7, 2: len(d) - 6, 3: len(d) - 3, 4: len(d) - 1}
    done_d = [len([f for f in d if f not in queue[at[0] :]])]
    for j, dz in enumerate(order):
        while done_d[0] < max(need[dz], ahead.get(j, len(d))):
            run(d[done_d[0]])
            done_d[0] += 1
        phase("q_have")
        D.have(dz)
        phase("q_dot")
        zs = zat(dz)
        part = dot(hid[...], dnbuf[pl.ds(pl.multiple_of(zs * 256, 256), 256), :], ((1,), (1,)))
        for i in range(4):
            pown[j % 2, i * 64 : i * 64 + 64, :] = part[i * 128 : i * 128 + 64]
            psend[j, i * 64 : i * 64 + 64, :] = part[i * 128 + 64 : i * 128 + 128].astype(BF16)
        DD[j].start()
        if j > 0:
            combine(j - 1, zat(order[j - 1]))
    combine(7, zat(4))

    phase("p_last")
    for j, dz in enumerate(order):
        cols = pl.ds(pl.multiple_of(zat(dz) * 256, 256), 256)
        phase("q_rswait")
        for k in (1, 2, 3):
            RS[j][k - 1].wait()
        phase("q_fin")
        fin[:, cols] = fin[:, cols] + (yrecv[j, 1].astype(F32) + yrecv[j, 2].astype(F32) + yrecv[j, 3].astype(F32))
    summed = RESIDUAL_SCALE * xbuf[0:64, :].astype(F32) + fin[...]
    out_ref[...] = layer_norm(summed, sg_ref[...], sb_ref[...]).astype(BF16)
    phase("p_drain")
    for t in pool.all:
        t.drain()
    phase(None)


def per_device(
    queries, keys, values, residual, query_gain, key_gain, out_weight, first_gain, first_bias, up_weight, down_weight,
    second_gain, second_bias,
):
    cos, sin = rotary_tables()
    zero = np.zeros((256, 64), np.float32)

    def table(t):
        return jnp.asarray(np.concatenate([t, zero], 1)), jnp.asarray(np.concatenate([zero, t], 1)[:GRID_W])

    vmem, hbm = pl.BlockSpec(memory_space=pltpu.VMEM), pl.BlockSpec(memory_space=pl.ANY)
    scratch = [
        pltpu.VMEM((KEYS, 128), BF16),
        pltpu.VMEM((128, KEYS), BF16),
        pltpu.VMEM((2048, 128), BF16),
        pltpu.VMEM((8, 128, 256), F32),
        pltpu.VMEM((8, 8, 256), F32),
        pltpu.VMEM((8, 8, 256), F32),
        pltpu.VMEM((1536, 256), F32),
        pltpu.VMEM((1536, 256), F32),
        pltpu.VMEM((4, 2, 128, 256), BF16),
        pltpu.VMEM((4, 2, 128, 256), BF16),
        pltpu.VMEM((4, 2, 8, 256), F32),
        pltpu.VMEM((4, 2, 8, 256), F32),
        pltpu.VMEM((256, 256), BF16),
        pltpu.VMEM((4, 64, 256), BF16),
        pltpu.VMEM((1024, 2048), BF16),
        pltpu.VMEM((64, 2048), BF16),
        pltpu.VMEM((512, 2048), BF16),
        pltpu.VMEM((2048, W_COLS), BF16),
        pltpu.VMEM((2048, W_COLS), BF16),
        pltpu.VMEM((512, W_COLS), BF16),
        pltpu.VMEM((8, 256, 256), BF16),
        pltpu.VMEM((8, 256, 256), BF16),
        pltpu.VMEM((2, 256, 256), F32),
        pltpu.VMEM((8, 4, 64, 256), BF16),
        pltpu.VMEM((8, 4, 64, 256), BF16),
        pltpu.VMEM((64, 2048), F32),
        pltpu.SemaphoreType.DMA((N_SEMS,)),
        pltpu.SemaphoreType.DMA((N_SEMS,)),
        pltpu.SemaphoreType.DMA((4,)),
    ]
    return pl.pallas_call(
        kernel,
        out_shape=jax.ShapeDtypeStruct((64, 2048), BF16),
        in_specs=[vmem] * 13 + [hbm] * 4,
        out_specs=vmem,
        scratch_shapes=scratch,
        compiler_params=pltpu.CompilerParams(collective_id=0, has_side_effects=True, vmem_limit_bytes=62 * 1024 * 1024),
        name="layer",
    )(
        queries, keys, values, *table(cos), *table(sin), query_gain[None], key_gain[None], first_gain[None], first_bias[None],
        second_gain[None], second_bias[None], residual, out_weight, up_weight, down_weight,
    )


def solution(mesh):
    in_specs = (
        P("sp", "tp"), P("sp", "tp"), P("sp", "tp"), P(("sp", "tp"), None), P(), P(), P(), P(), P(),
        P("sp", "tp"), P("sp", "tp"), P(), P(),
    )
    return jax.shard_map(per_device, mesh=mesh, in_specs=in_specs, out_specs=P(("sp", "tp"), None), check_vma=False)
```
